1024 devices in a mesh: sp: 128 (over z, y), tp: 8 (over x, core).
Axes of the slice: x: 4, y: 8, z: 16, core: 2. Of those that a mesh axis runs over, the one named last changes fastest.
Arguments:
- target: bfloat16 [896, 2048], P('sp'), may hold values from -6 to 6
- source: bfloat16 [32768, 2048], P('sp'), may hold values from -6 to 6
- tgt_gain: float32 [2, 2048], replicated, may hold values from 0.1 to 1.9
- src_gain: float32 [2, 2048], replicated, may hold values from 0.1 to 1.9
- w_query: bfloat16 [2, 2048, 2048], P(None, None, 'tp'), may hold values from -0.125 to 0.125
- w_key: bfloat16 [2, 2048, 2048], P(None, None, 'tp'), may hold values from -0.125 to 0.125
- w_value: bfloat16 [2, 2048, 2048], P(None, None, 'tp'), may hold values from -0.125 to 0.125
- w_out: bfloat16 [2, 2048, 2048], P(None, 'tp'), may hold values from -0.125 to 0.125
- score_scale: float32 [2, 8], P(None, 'tp'), may hold values from 1.5 to 4
Outputs:
- result: bfloat16 [896, 2048], P('sp')
The draws below stay inside these ranges and needn't reach their ends.
All inputs are finite; a program needn't handle non-finite values.
Results may differ from the reference program's by a relative error of at most 0.015.
Values may be sent and summed in bfloat16 or wider, within the bound.
A program may use at most 64 MiB of HBM per device.

```python
import math
import jax
import jax.numpy as jnp
from jax import lax

D = 2048
HEADS = 8
HEAD_DIM = 256
LAYERS = 2
SOURCE = 32768
TOKENS = 896
N_TP = 8


def level_of(rng, shape, cuts, least, top_value):
    factor_of, own = 1.0, jax.random.fold_in(rng, 6)
    for dim, parts in cuts:
        draws = jnp.exp(jax.random.uniform(jax.random.fold_in(own, dim), (parts,), jnp.float32, least / len(cuts), top_value / len(cuts)))
        factor_of = factor_of * jnp.repeat(draws, shape[dim] // parts).reshape([-1 if axis == dim else 1 for axis in range(len(shape))])
    return factor_of


def noise(stream_key, shape, deviation, reach, split=(), kind=jnp.bfloat16):
    array = jax.random.normal(stream_key, shape, jnp.float32) * deviation
    if len(split) > 0:
        array = level_of(stream_key, shape, split, -0.22, 0.18) * array
    return jnp.clip(array, min=-reach, max=reach).astype(kind)


def setup_inputs(seed: int = 0) -> dict:
    arg_keys = jax.random.split(jax.random.key(seed), 10)
    target = noise(arg_keys[0], (TOKENS, D), 1.0, 6.0, ((0, 128),))
    source = noise(arg_keys[1], (SOURCE, D), 1.0, 6.0, ((0, 128),))
    tgt_gain = jnp.clip(1.0 + 0.18 * jax.random.normal(arg_keys[2], (LAYERS, D), jnp.float32), 0.1, 1.9)
    src_gain = jnp.clip(1.0 + 0.18 * jax.random.normal(arg_keys[3], (LAYERS, D), jnp.float32), 0.1, 1.9)
    w_query = noise(arg_keys[4], (LAYERS, D, HEADS * HEAD_DIM), D ** -0.5, 0.125, ((2, 8),))
    w_key = noise(arg_keys[5], (LAYERS, D, HEADS * HEAD_DIM), D ** -0.5, 0.125, ((2, 8),))
    w_value = noise(arg_keys[6], (LAYERS, D, HEADS * HEAD_DIM), D ** -0.5, 0.125, ((2, 8),))
    w_out = noise(arg_keys[7], (LAYERS, HEADS * HEAD_DIM, D), (HEADS * HEAD_DIM) ** -0.5, 0.125, ((1, 8),))
    score_scale = jnp.clip(jnp.exp(math.log(4.0) - 0.98082925 * jax.random.uniform(arg_keys[8], (LAYERS, HEADS), jnp.float32) ** level_of(arg_keys[8], (LAYERS, HEADS), ((1, 8),), -0.2, 0.2)), 1.5, 4.0)
    return {"target": target, "source": source, "tgt_gain": tgt_gain, "src_gain": src_gain, "w_query": w_query, "w_key": w_key, "w_value": w_value, "w_out": w_out, "score_scale": score_scale}


EPS = 1e-06

def row_scale(values):
    return lax.rsqrt(lax.optimization_barrier(jnp.mean(values * values, axis=-1, keepdims=True)) + EPS)

def head_norm(projected):
    heads = projected.reshape(projected.shape[0], -1, HEAD_DIM)
    heads = heads * row_scale(heads)
    return heads.reshape(projected.shape).astype(jnp.bfloat16)

def reference(target, source, tgt_gain, src_gain, w_query, w_key, w_value, w_out, score_scale):
    root = math.sqrt(HEAD_DIM)
    src_float = source.astype(jnp.float32)
    src_scale = row_scale(src_float)
    hidden = target
    group_heads = HEADS // N_TP
    for layer_index in range(LAYERS):
        normed_src = (src_float * src_scale * src_gain[layer_index]).astype(jnp.bfloat16)
        keys = head_norm(jnp.dot(normed_src, w_key[layer_index], preferred_element_type=jnp.float32))
        values = jnp.dot(normed_src, w_value[layer_index], preferred_element_type=jnp.float32).astype(jnp.bfloat16)
        hidden_float = hidden.astype(jnp.float32)
        normed_tgt = (hidden_float * row_scale(hidden_float) * tgt_gain[layer_index]).astype(jnp.bfloat16)
        queries = head_norm(jnp.dot(normed_tgt, w_query[layer_index], preferred_element_type=jnp.float32))
        query_heads = queries.reshape(TOKENS, HEADS, HEAD_DIM).transpose(1, 0, 2)
        key_heads = keys.reshape(SOURCE, HEADS, HEAD_DIM).transpose(1, 0, 2)
        value_heads = values.reshape(SOURCE, HEADS, HEAD_DIM).transpose(1, 0, 2)

        def one_head(inputs):
            query_one, key_one, value_one, scale_one = inputs
            scores = jnp.dot(query_one, key_one.T, preferred_element_type=jnp.float32)
            logits = scale_one * (scores / root - root)
            weights = jnp.exp(logits)
            denominators = lax.optimization_barrier(jnp.sum(weights, axis=1))
            numerators = jnp.dot(weights.astype(jnp.bfloat16), value_one, preferred_element_type=jnp.float32)
            return (numerators / denominators[:, None]).astype(jnp.bfloat16)
        outputs = lax.map(one_head, (query_heads, key_heads, value_heads, score_scale[layer_index]))
        attended = outputs.transpose(1, 0, 2).reshape(TOKENS, HEADS * HEAD_DIM)
        branch = jnp.zeros((TOKENS, D), jnp.float32)
        group_width = group_heads * HEAD_DIM
        for group in range(N_TP):
            columns = attended[:, group * group_width:(group + 1) * group_width]
            rows_out = w_out[layer_index, group * group_width:(group + 1) * group_width, :]
            share = jnp.dot(columns, rows_out, preferred_element_type=jnp.float32).astype(jnp.bfloat16)
            branch = branch + share.astype(jnp.float32)
        hidden = (hidden_float + branch).astype(jnp.bfloat16)
    return hidden
```

```python
import functools
import math

import jax
import jax.numpy as jnp
from jax import lax
from jax.experimental import pallas as pl
from jax.experimental.pallas import tpu as pltpu
from jax.sharding import Mesh
from jax.sharding import PartitionSpec as P

HEAD_DIM = 256
ROOT = math.sqrt(HEAD_DIM)
EPS = 1e-06
PAD = 8
MESH = pl.DeviceIdType.MESH
BF16 = jnp.bfloat16
F32 = jnp.float32


def row_scale(values):
    return lax.rsqrt(jnp.mean(values * values, axis=-1, keepdims=True) + EPS)


def dot_nt(a, b):
    return lax.dot_general(a, b, (((1,), (1,)), ((), ())), preferred_element_type=F32)


def kernel(
    sizes,
    target,
    source,
    tgt_gain,
    src_gain,
    w_query,
    w_key,
    w_value,
    w_out,
    score_scale,
    out,
    hid,
    src,
    tgt,
    tgain,
    sgain,
    wq,
    wk,
    wv,
    wo,
    scl,
    ns,
    kv,
    qall,
    nacc,
    dacc,
    nsend,
    nrecv,
    share,
    load_sem,
    kv_send,
    kv_recv,
    q_send,
    q_recv,
    n_send,
    n_recv,
    t_send,
    t_recv,
):
    nz, ny, nt = sizes
    half = ny // 2
    z, y, t = lax.axis_index("z"), lax.axis_index("y"), lax.axis_index("tp")
    layers = wq.shape[0]
    rows = src.shape[0]
    toks = target.shape[0]
    tall = nz * PAD

    loads = [
        pltpu.make_async_copy(a, b, load_sem.at[i])
        for i, (a, b) in enumerate(
            [
                (source, src),
                (src_gain, sgain),
                (w_key.at[0], wk.at[0]),
                (w_value.at[0], wv.at[0]),
                (target, tgt),
                (tgt_gain, tgain),
                (score_scale, scl),
                (w_query.at[0], wq.at[0]),
                (w_key.at[1], wk.at[1]),
                (w_value.at[1], wv.at[1]),
                (w_out.at[0], wo.at[0]),
                (w_query.at[1], wq.at[1]),
                (w_out.at[1], wo.at[1]),
            ]
        )
    ]
    for load in loads:
        load.start()

    barrier = pltpu.get_barrier_semaphore()
    right, left = lax.rem(y + 1, ny), lax.rem(y + ny - 1, ny)

    def greet_z(k, carry):
        pl.semaphore_signal(barrier, inc=1, device_id={"z": lax.rem(z + k, nz)}, device_id_type=MESH)
        return carry

    def greet_t(k, carry):
        pl.semaphore_signal(barrier, inc=1, device_id={"tp": lax.rem(t + k, nt)}, device_id_type=MESH)
        return carry

    lax.fori_loop(1, nz, greet_z, 0)
    pl.semaphore_signal(barrier, inc=1, device_id={"y": right}, device_id_type=MESH)
    pl.semaphore_signal(barrier, inc=1, device_id={"y": left}, device_id_type=MESH)
    lax.fori_loop(1, nt, greet_t, 0)

    loads[0].wait()
    loads[1].wait()
    step = 16

    def norm_rows(i, carry):
        at = pl.ds(pl.multiple_of(i * step, step), step)
        x = src[at, :].astype(F32)
        x = x * row_scale(x)
        for layer in range(layers):
            ns[layer, at, :] = (x * sgain[layer : layer + 1, :]).astype(BF16)
        return carry

    lax.fori_loop(0, rows // step, norm_rows, 0)

    def source_side(layer):
        normed = ns[layer]
        keys = jnp.dot(normed, wk[layer], preferred_element_type=F32)
        kv[layer, 0, 0] = (keys * row_scale(keys)).astype(BF16)
        kv[layer, 1, 0] = jnp.dot(normed, wv[layer], preferred_element_type=F32).astype(BF16)

    def queries_of(layer):
        hidden = hid[...]
        normed = (hidden * row_scale(hidden) * tgain[layer : layer + 1, :]).astype(BF16)
        queries = jnp.dot(normed, wq[layer], preferred_element_type=F32)
        qall[layer, 0] = (queries * row_scale(queries)).astype(BF16)

    loads[2].wait()
    loads[3].wait()
    source_side(0)
    for i in (4, 5, 6, 7):
        loads[i].wait()
    hid[...] = jnp.zeros_like(hid)
    hid[0:toks, :] = tgt[...].astype(F32)
    queries_of(0)
    loads[8].wait()
    loads[9].wait()
    source_side(1)
    for i in (10, 11, 12):
        loads[i].wait()

    pl.semaphore_wait(barrier, nz - 1 + 2 + nt - 1)

    def ring(layer, which, step):
        copies = []
        for way, peer in ((0, right), (1, left)):
            if step == half - 1 and which != way:
                continue
            held = 0 if step == 0 else (step if way == 0 else half + step)
            lands = half if step == half - 1 else (step + 1 if way == 0 else half + step + 1)
            copies.append(
                pltpu.make_async_remote_copy(
                    src_ref=kv.at[layer, which, held],
                    dst_ref=kv.at[layer, which, lands],
                    send_sem=kv_send.at[layer, which, way, step],
                    recv_sem=kv_recv.at[layer, which, lands],
                    device_id={"y": peer},
                    device_id_type=MESH,
                )
            )
        return copies

    def ring_start(layer, which, step):
        for copy in ring(layer, which, step):
            copy.start()

    def ring_arrived(layer, which, step):
        for copy in ring(layer, which, step):
            copy.wait_recv()

    def ring_next(layer, which, step):
        ring_arrived(layer, which, step)
        if step < half - 1:
            for copy in ring(layer, which, step + 1):
                copy.start()

    def far_first(k):
        return k

    def z_order(i):
        away = (i + 1) // 2
        side = lax.rem(i, 2)
        return nz // 2 + jnp.where(side == 1, away, -away)

    def q_copy(layer, k):
        return pltpu.make_async_remote_copy(
            src_ref=qall.at[layer, 0],
            dst_ref=qall.at[layer, nz - k],
            send_sem=q_send.at[layer],
            recv_sem=q_recv.at[layer],
            device_id={"z": lax.rem(z + k, nz)},
            device_id_type=MESH,
        )

    def q_start(layer):
        def go(i, carry):
            q_copy(layer, z_order(i)).start()
            return carry

        lax.fori_loop(0, nz - 1, go, 0)

    def wait_all(ref, send, recv):
        both = pltpu.make_async_remote_copy(
            src_ref=ref,
            dst_ref=ref,
            send_sem=send,
            recv_sem=recv,
            device_id={"z": lax.rem(z + 1, nz)},
            device_id_type=MESH,
        )
        both.wait_recv()
        return both

    def n_start(layer):
        def go(i, carry):
            k = z_order(i)
            pltpu.make_async_remote_copy(
                src_ref=nsend.at[layer, k],
                dst_ref=nrecv.at[layer, nz - k],
                send_sem=n_send.at[layer],
                recv_sem=n_recv.at[layer],
                device_id={"z": lax.rem(z + k, nz)},
                device_id_type=MESH,
            ).start()
            return carry

        lax.fori_loop(0, nz - 1, go, 0)

    def attend(layer, slot):
        scores = dot_nt(qall[layer].reshape(tall, HEAD_DIM), kv[layer, 0, slot])
        weights = jnp.exp(scl[layer : layer + 1, :] * (scores * (1.0 / ROOT) - ROOT))
        sums = weights[:, 0:128]
        for c in range(128, rows, 128):
            sums = sums + weights[:, c : c + 128]
        dacc[...] += sums
        nacc[...] += jnp.dot(weights.astype(BF16), kv[layer, 1, slot], preferred_element_type=F32)

    def partials(layer):
        denoms = jnp.sum(dacc[...].T, axis=0, keepdims=True)
        upper = denoms.astype(BF16).astype(F32)
        lower = denoms - upper
        pad = jnp.zeros((1, 128 - tall), F32)
        parts = [upper, lower] if tall == 128 else [upper, pad, lower, pad]
        extra = jnp.concatenate(parts, axis=1).reshape(1, 1, 256)
        shape = (nz, PAD, HEAD_DIM)
        lane = lax.rem(lax.broadcasted_iota(jnp.int32, shape, 2), 128)
        block = lax.broadcasted_iota(jnp.int32, shape, 0)
        row = lax.broadcasted_iota(jnp.int32, shape, 1)
        mine = jnp.where(lane // PAD == block, jnp.broadcast_to(extra, shape), 0.0)
        full = jnp.where(row == PAD - 1, mine, nacc[...].reshape(shape)).astype(BF16)
        nsend[layer] = full
        nrecv[layer, 0] = full[0]

    def share_of(layer):
        total = jnp.sum(nrecv[layer].astype(F32), axis=0)
        shape = (PAD, 128)
        lane = lax.broadcasted_iota(jnp.int32, shape, 1)
        row = lax.broadcasted_iota(jnp.int32, shape, 0)
        both = total[PAD - 1 : PAD, 0:128] + total[PAD - 1 : PAD, 128:256]
        denoms = jnp.sum(
            jnp.where(lax.rem(lane, PAD) == row, jnp.broadcast_to(both, shape), 0.0),
            axis=1,
            keepdims=True,
        )
        real = lax.broadcasted_iota(jnp.int32, (PAD, HEAD_DIM), 0) < toks
        attended = jnp.where(real, total / denoms, 0.0).astype(BF16)
        share[layer, 0] = jnp.dot(attended, wo[layer], preferred_element_type=F32).astype(BF16)

    def t_copy(layer, k):
        return pltpu.make_async_remote_copy(
            src_ref=share.at[layer, 0],
            dst_ref=share.at[layer, nt - k],
            send_sem=t_send.at[layer],
            recv_sem=t_recv.at[layer],
            device_id={"tp": lax.rem(t + k, nt)},
            device_id_type=MESH,
        )

    def t_start(layer):
        for k in sorted(range(1, nt), key=lambda k: abs(k - nt // 2)):
            t_copy(layer, k).start()

    def add_branch(layer):
        branch = share[layer, 0].astype(F32)
        for k in range(1, nt):
            branch = branch + share[layer, k].astype(F32)
        return (hid[...] + branch).astype(BF16)

    def clear():
        nacc[...] = jnp.zeros_like(nacc)
        dacc[...] = jnp.zeros_like(dacc)

    q_start(0)
    ring_start(0, 0, 0)
    ring_start(0, 1, 0)
    clear()
    waits = []
    for s in range(half):
        ring_next(0, 0, s)
        ring_next(0, 1, s)
        if s == half - 2:
            ring_start(1, 0, 0)
            ring_start(1, 1, 0)
        if s == 0:
            waits.append(wait_all(qall.at[0, pl.ds(1, nz - 1)], q_send.at[0], q_recv.at[0]))
            attend(0, 0)
        if s < half - 1:
            attend(0, s + 1)
            attend(0, half + s + 1)
        else:
            attend(0, half)
    partials(0)
    n_start(0)
    ring_next(1, 0, 0)
    ring_next(1, 1, 0)
    waits.append(wait_all(nrecv.at[0, pl.ds(1, nz - 1)], n_send.at[0], n_recv.at[0]))
    share_of(0)
    t_start(0)
    ring_next(1, 0, 1)
    ring_next(1, 1, 1)
    waits.append(wait_all(share.at[0, pl.ds(1, nt - 1)], t_send.at[0], t_recv.at[0]))
    hid[...] = add_branch(0).astype(F32)
    queries_of(1)
    q_start(1)
    clear()
    for s in range(2, half):
        ring_next(1, 0, s)
        ring_next(1, 1, s)
    waits.append(wait_all(qall.at[1, pl.ds(1, nz - 1)], q_send.at[1], q_recv.at[1]))

    def attend_slot(slot, carry):
        attend(1, slot)
        return carry

    lax.fori_loop(0, ny, attend_slot, 0)
    partials(1)
    n_start(1)
    waits.append(wait_all(nrecv.at[1, pl.ds(1, nz - 1)], n_send.at[1], n_recv.at[1]))
    share_of(1)
    t_start(1)
    waits.append(wait_all(share.at[1, pl.ds(1, nt - 1)], t_send.at[1], t_recv.at[1]))
    out[...] = add_branch(1)[0:toks, :]

    for both in waits:
        both.wait_send()
    for layer in range(layers):
        for s in range(half):
            for which in (0, 1):
                for copy in ring(layer, which, s):
                    copy.wait_send()


def body(sizes, *arrays):
    target, source = arrays[0], arrays[1]
    w_query, w_out = arrays[4], arrays[7]
    nz, ny, nt = sizes
    toks, width = target.shape
    rows = source.shape[0]
    layers = w_query.shape[0]
    half = ny // 2
    hbm = pl.BlockSpec(memory_space=pl.ANY)
    vmem = pltpu.VMEM
    dma = pltpu.SemaphoreType.DMA
    return pl.pallas_call(
        functools.partial(kernel, sizes),
        out_shape=jax.ShapeDtypeStruct((toks, width), BF16),
        in_specs=[hbm] * 9,
        out_specs=pl.BlockSpec(memory_space=pltpu.VMEM),
        scratch_shapes=[
            vmem((PAD, width), F32),
            vmem((rows, width), BF16),
            vmem((toks, width), BF16),
            vmem((layers, width), F32),
            vmem((layers, width), F32),
            vmem((layers, width, HEAD_DIM), BF16),
            vmem((layers, width, HEAD_DIM), BF16),
            vmem((layers, width, HEAD_DIM), BF16),
            vmem((layers, HEAD_DIM, width), BF16),
            vmem((layers, 1), F32),
            vmem((layers, rows, width), BF16),
            vmem((layers, 2, ny, rows, HEAD_DIM), BF16),
            vmem((layers, nz, PAD, HEAD_DIM), BF16),
            vmem((nz * PAD, HEAD_DIM), F32),
            vmem((nz * PAD, 128), F32),
            vmem((layers, nz, PAD, HEAD_DIM), BF16),
            vmem((layers, nz, PAD, HEAD_DIM), BF16),
            vmem((layers, nt, PAD, width), BF16),
            dma((13,)),
            dma((layers, 2, 2, half)),
            dma((layers, 2, ny)),
            dma((layers,)),
            dma((layers,)),
            dma((layers,)),
            dma((layers,)),
            dma((layers,)),
            dma((layers,)),
        ],
        compiler_params=pltpu.CompilerParams(collective_id=0, has_side_effects=True),
    )(*arrays)


SP = ("z", "y")


def torus_of(mesh):
    return Mesh(mesh.devices.reshape(16, 8, mesh.shape["tp"]), ("z", "y", "tp"))


def on_torus(torus):
    sizes = tuple(torus.shape[a] for a in ("z", "y", "tp"))
    return jax.shard_map(
        functools.partial(body, sizes),
        mesh=torus,
        in_specs=(
            P(SP, None),
            P(SP, None),
            P(),
            P(),
            P(None, None, "tp"),
            P(None, None, "tp"),
            P(None, None, "tp"),
            P(None, "tp", None),
            P(None, "tp"),
        ),
        out_specs=P(SP, None),
        check_vma=False,
    )


def solution(mesh):
    return on_torus(torus_of(mesh))
```

```python
import functools
import math

import jax
import jax.numpy as jnp
from jax import lax
from jax.experimental import pallas as pl
from jax.experimental.pallas import tpu as pltpu
from jax.sharding import Mesh
from jax.sharding import PartitionSpec as P

HEAD_DIM = 256
ROOT = math.sqrt(HEAD_DIM)
EPS = 1e-06
PAD = 8
MESH = pl.DeviceIdType.MESH
scope = jax.named_scope
BF16 = jnp.bfloat16
F32 = jnp.float32


def row_scale(values):
    return lax.rsqrt(jnp.mean(values * values, axis=-1, keepdims=True) + EPS)


def dot_nt(a, b):
    return lax.dot_general(a, b, (((1,), (1,)), ((), ())), preferred_element_type=F32)


def kernel(
    sizes,
    target,
    source,
    tgt_gain,
    src_gain,
    w_query,
    w_key,
    w_value,
    w_out,
    score_scale,
    out,
    hid,
    src,
    scale_of,
    tgt,
    tgain,
    sgain,
    wq,
    wk,
    wv,
    wo,
    scl,
    ns,
    kv0,
    kv1,
    q0,
    q1,
    nsend0,
    nrecv0,
    nsend1,
    nrecv1,
    share,
    load_sem,
    kv0_send,
    kv0_recv,
    kv1_send,
    kv1_recv,
    q_send,
    q_recv,
    n_send,
    n_recv,
    t_send,
    t_recv,
):
    nz, ny, nt = sizes
    half = ny // 2
    z, y, t = lax.axis_index("z"), lax.axis_index("y"), lax.axis_index("tp")
    layers = wq.shape[0]
    rows = src.shape[0]
    toks = target.shape[0]
    tall = nz * PAD

    def line(dy):
        return lax.rem(y + (dy + ny), ny)

    def plane(k):
        return lax.rem(z + k, nz)

    def load(i, a, b):
        return pltpu.make_async_copy(a, b, load_sem.at[i])

    first = [
        load(0, source, src),
        load(1, src_gain, sgain),
        load(2, w_key.at[0], wk.at[0]),
        load(3, w_value.at[0], wv.at[0]),
    ]
    later = [
        load(4, target, tgt),
        load(5, tgt_gain, tgain),
        load(6, w_query.at[0], wq.at[0]),
        load(7, score_scale, scl),
        load(8, w_key.at[1], wk.at[1]),
        load(9, w_value.at[1], wv.at[1]),
        load(10, w_out.at[0], wo.at[0]),
        load(11, w_query.at[1], wq.at[1]),
        load(12, w_out.at[1], wo.at[1]),
    ]
    for one in first:
        one.start()

    barrier = pltpu.get_barrier_semaphore()

    def greet(peer):
        pl.semaphore_signal(barrier, inc=1, device_id=peer, device_id_type=MESH)

    sides = (2, -2)
    for dy in (1, -1) + sides:
        greet({"y": line(dy)})
    for k in range(1, nt):
        greet({"tp": lax.rem(t + k, nt)})

    def greet_planes(k, carry):
        greet({"z": plane(k)})
        for dy in sides:
            greet({"z": plane(k), "y": line(dy)})
        return carry

    lax.fori_loop(1, nz, greet_planes, 0)
    greeted = 4 + nt - 1 + (nz - 1) * 3
    for one in later:
        one.start()

    step = 16

    def at_rows(i):
        return pl.ds(pl.multiple_of(i * step, step), step)

    def squares(i, carry):
        for u in range(2):
            x = src[at_rows(2 * i + u), :].astype(F32)
            x = x * x
            total = x[:, 0:128]
            for c in range(128, x.shape[1], 128):
                total = total + x[:, c : c + 128]
            scale_of[at_rows(2 * i + u), :] = total
        return carry

    def norm_rows(layer):
        def go(i, carry):
            for u in range(2):
                at = at_rows(2 * i + u)
                x = src[at, :].astype(F32) * scale_of[at, 0:1]
                ns[at, :] = (x * sgain[layer : layer + 1, :]).astype(BF16)
            return carry

        lax.fori_loop(0, rows // (2 * step), go, 0)

    def keys_of(layer):
        keys = jnp.dot(ns[...], wk[layer], preferred_element_type=F32)
        return (keys * row_scale(keys)).astype(BF16)

    def values_of(layer):
        return jnp.dot(ns[...], wv[layer], preferred_element_type=F32).astype(BF16)

    def queries_of(layer):
        hidden = hid[...]
        normed = (hidden * row_scale(hidden) * tgain[layer : layer + 1, :]).astype(BF16)
        queries = jnp.dot(normed, wq[layer], preferred_element_type=F32)
        return (queries * row_scale(queries)).astype(BF16)

    def push(src_ref, dst_ref, send, recv, peer):
        return pltpu.make_async_remote_copy(
            src_ref=src_ref,
            dst_ref=dst_ref,
            send_sem=send,
            recv_sem=recv,
            device_id=peer,
            device_id_type=MESH,
        )

    sign = 1 - 2 * lax.rem(t, 2)
    ahead, behind = lax.rem(y + sign + ny, ny), lax.rem(y - sign + ny, ny)

    def near(which, held, lands):
        return push(
            kv0.at[which, held],
            kv0.at[which, lands],
            kv0_send.at[which, lands],
            kv0_recv.at[which, lands],
            {"y": ahead if lands == 3 else behind},
        )

    right, left = line(1), line(-1)

    def ring(which, step):
        copies = []
        for way, peer in ((0, right), (1, left)):
            if step == half - 1 and which != way:
                continue
            held = 0 if step == 0 else (step if way == 0 else half + step)
            lands = half if step == half - 1 else (step + 1 if way == 0 else half + step + 1)
            copies.append(
                push(
                    kv1.at[which, held],
                    kv1.at[which, lands],
                    kv1_send.at[which, way, step],
                    kv1_recv.at[which, lands],
                    {"y": peer},
                )
            )
        return copies

    def ring_next(step):
        for which in (0, 1):
            for copy in ring(which, step):
                copy.wait_recv()
            if step < half - 1:
                for copy in ring(which, step + 1):
                    copy.start()

    def z_order(i):
        away = (i + 1) // 2
        return lax.rem(nz // 2 + jnp.where(lax.rem(i, 2) == 1, away, -away), nz)

    def q0_start():
        def go(i, carry):
            k = z_order(i)
            for d in range(2):
                push(
                    q0.at[2, 0],
                    q0.at[d, lax.rem(nz - k, nz)],
                    q_send.at[0],
                    q_recv.at[0],
                    {"z": plane(k), "y": line(sides[d])},
                ).start()
            return carry

        lax.fori_loop(0, nz, go, 0)

    def n0_start(d):
        def go(i, carry):
            k = z_order(i)
            push(
                nsend0.at[d, k],
                nrecv0.at[d, lax.rem(nz - k, nz)],
                n_send.at[0],
                n_recv.at[0],
                {"z": plane(k), "y": line(-sides[d])},
            ).start()
            return carry

        lax.fori_loop(0, nz, go, 0)

    def q1_start():
        def go(i, carry):
            k = z_order(i)
            push(q1.at[0], q1.at[nz - k], q_send.at[1], q_recv.at[1], {"z": plane(k)}).start()
            return carry

        lax.fori_loop(0, nz - 1, go, 0)

    def n1_start():
        def go(i, carry):
            k = z_order(i)
            push(
                nsend1.at[k], nrecv1.at[nz - k], n_send.at[1], n_recv.at[1], {"z": plane(k)}
            ).start()
            return carry

        lax.fori_loop(0, nz - 1, go, 0)

    def t_start(layer):
        for k in sorted(range(1, nt), key=lambda k: abs(k - nt // 2)):
            push(
                share.at[layer, 0],
                share.at[layer, nt - k],
                t_send.at[layer],
                t_recv.at[layer],
                {"tp": lax.rem(t + k, nt)},
            ).start()

    waits = []

    def wait_all(ref, send, recv, peer):
        both = push(ref, ref, send, recv, peer)
        both.wait_recv()
        waits.append(both)

    def weigh(layer, queries, keys):
        scores = dot_nt(queries, keys)
        weights = jnp.exp(scl[layer] * (scores * (1.0 / ROOT) - ROOT))
        sums = weights[:, 0:128]
        for c in range(128, weights.shape[1], 128):
            sums = sums + weights[:, c : c + 128]
        return weights.astype(BF16), sums

    def with_denominators(numer, sums):
        denoms = jnp.sum(sums.T, axis=0, keepdims=True)
        upper = denoms.astype(BF16).astype(F32)
        lower = denoms - upper
        pad = jnp.zeros((1, 128 - tall), F32)
        parts = [upper, lower] if tall == 128 else [upper, pad, lower, pad]
        extra = jnp.concatenate(parts, axis=1).reshape(1, 1, 256)
        shape = (nz, PAD, HEAD_DIM)
        lane = lax.rem(lax.broadcasted_iota(jnp.int32, shape, 2), 128)
        block = lax.broadcasted_iota(jnp.int32, shape, 0)
        row = lax.broadcasted_iota(jnp.int32, shape, 1)
        mine = jnp.where(lane // PAD == block, jnp.broadcast_to(extra, shape), 0.0)
        return jnp.where(row == PAD - 1, mine, numer.reshape(shape)).astype(BF16)

    def share_of(layer, total):
        shape = (PAD, 128)
        lane = lax.broadcasted_iota(jnp.int32, shape, 1)
        row = lax.broadcasted_iota(jnp.int32, shape, 0)
        both = total[PAD - 1 : PAD, 0:128] + total[PAD - 1 : PAD, 128:256]
        denoms = jnp.sum(
            jnp.where(lax.rem(lane, PAD) == row, jnp.broadcast_to(both, shape), 0.0),
            axis=1,
            keepdims=True,
        )
        real = lax.broadcasted_iota(jnp.int32, (PAD, HEAD_DIM), 0) < toks
        attended = jnp.where(real, total / denoms, 0.0).astype(BF16)
        share[layer, 0] = jnp.dot(attended, wo[layer], preferred_element_type=F32).astype(BF16)

    def add_branch(layer):
        branch = share[layer, 0].astype(F32)
        for k in range(1, nt):
            branch = branch + share[layer, k].astype(F32)
        return (hid[...] + branch).astype(BF16)

    with scope("load"):
        first[0].wait()
    with scope("norm"):
        lax.fori_loop(0, rows // (2 * step), squares, 0)
        mean = jnp.sum(scale_of[...], axis=-1, keepdims=True) * (1.0 / src.shape[1])
        scale_of[...] = jnp.broadcast_to(lax.rsqrt(mean + EPS), scale_of.shape)
        first[1].wait()
        norm_rows(0)
    with scope("keys_0"):
        first[2].wait()
        kv0[0, 0] = keys_of(0)
    with scope("barrier"):
        pl.semaphore_wait(barrier, greeted)
    near(0, 0, 1).start()
    near(0, 0, 3).start()
    with scope("values_0"):
        first[3].wait()
        kv0[1, 0] = values_of(0)
    near(1, 0, 1).start()
    near(1, 0, 3).start()
    with scope("queries_0"):
        for i in (0, 1, 2):
            later[i].wait()
        hid[...] = jnp.zeros_like(hid)
        hid[0:toks, :] = tgt[...].astype(F32)
        q0[2, 0] = queries_of(0)
        q0_start()
    with scope("source_1"):
        norm_rows(1)
        for i in (3, 4, 5):
            later[i].wait()
        kv1[0, 0] = keys_of(1)
        kv1[1, 0] = values_of(1)
        for i in (6, 7, 8):
            later[i].wait()
    for which in (0, 1):
        with scope(f"near_0_{which}"):
            near(which, 0, 1).wait_recv()
            near(which, 1, 2).start()
            near(which, 0, 3).wait_recv()
    for which in (0, 1):
        for copy in ring(which, 0):
            copy.start()
    with scope("q_wait_0"):
        wait_all(
            q0.at[pl.ds(0, 2)], q_send.at[0], q_recv.at[0], {"z": plane(1), "y": line(2)}
        )
    numer = jnp.zeros((2 * tall, HEAD_DIM), F32)
    total = jnp.zeros((2 * tall, 128), F32)
    queries = q0[0:2].reshape(2 * tall, HEAD_DIM)
    for slot in (0, 1, 3, 2):
        if slot == 2:
            with scope("near_1_0"):
                near(0, 1, 2).wait_recv()
        with scope(f"attend_0_{slot}"):
            weights, sums = weigh(0, queries, kv0[0, slot])
            total = total + sums
        if slot == 2:
            with scope("near_1_1"):
                near(1, 1, 2).wait_recv()
        numer = numer + jnp.dot(weights, kv0[1, slot], preferred_element_type=F32)
    with scope("partials_0"):
        for d in range(2):
            at = slice(d * tall, (d + 1) * tall)
            nsend0[d] = with_denominators(numer[at], total[at])
            n0_start(d)
    with scope("ring_1_0"):
        ring_next(0)
    with scope("ring_1_1"):
        ring_next(1)
    with scope("n_wait_0"):
        wait_all(nrecv0, n_send.at[0], n_recv.at[0], {"z": plane(1), "y": line(2)})
    with scope("share_0"):
        share_of(0, jnp.sum(nrecv0[...].reshape(2 * nz, PAD, HEAD_DIM).astype(F32), axis=0))
        t_start(0)
    with scope("ring_1_2"):
        ring_next(2)
    with scope("t_wait_0"):
        others = {"tp": lax.rem(t + 1, nt)}
        wait_all(share.at[0, pl.ds(1, nt - 1)], t_send.at[0], t_recv.at[0], others)
    with scope("queries_1"):
        hid[...] = add_branch(0).astype(F32)
        q1[0] = queries_of(1)
        q1_start()
    with scope("ring_1_3"):
        ring_next(3)
    with scope("q_wait_1"):
        wait_all(q1.at[pl.ds(1, nz - 1)], q_send.at[1], q_recv.at[1], {"z": plane(1)})
    with scope("attend_1"):
        numer = jnp.zeros((tall, HEAD_DIM), F32)
        total = jnp.zeros((tall, 128), F32)
        queries = q1[...].reshape(tall, HEAD_DIM)
        for slot in range(0, ny, 2):
            keys = kv1[0, slot : slot + 2].reshape(2 * rows, HEAD_DIM)
            weights, sums = weigh(1, queries, keys)
            total = total + sums
            values = kv1[1, slot : slot + 2].reshape(2 * rows, HEAD_DIM)
            numer = numer + jnp.dot(weights, values, preferred_element_type=F32)
    with scope("partials_1"):
        full = with_denominators(numer, total)
        nsend1[...] = full
        nrecv1[0] = full[0]
        n1_start()
    with scope("n_wait_1"):
        wait_all(nrecv1.at[pl.ds(1, nz - 1)], n_send.at[1], n_recv.at[1], {"z": plane(1)})
    with scope("share_1"):
        share_of(1, jnp.sum(nrecv1[...].astype(F32), axis=0))
        t_start(1)
    with scope("t_wait_1"):
        wait_all(share.at[1, pl.ds(1, nt - 1)], t_send.at[1], t_recv.at[1], others)
    with scope("drain"):
        out[...] = add_branch(1)[0:toks, :]
        for both in waits:
            both.wait_send()
        for which in (0, 1):
            for held, lands in ((0, 1), (0, 3), (1, 2)):
                near(which, held, lands).wait_send()
            for s in range(half):
                for copy in ring(which, s):
                    copy.wait_send()


def body(sizes, *arrays):
    target, source = arrays[0], arrays[1]
    w_query = arrays[4]
    arrays = (*arrays[:8], arrays[8].reshape(-1))
    nz, ny, nt = sizes
    toks, width = target.shape
    rows = source.shape[0]
    layers = w_query.shape[0]
    half = ny // 2
    hbm = pl.BlockSpec(memory_space=pl.ANY)
    vmem = pltpu.VMEM
    dma = pltpu.SemaphoreType.DMA
    return pl.pallas_call(
        functools.partial(kernel, sizes),
        out_shape=jax.ShapeDtypeStruct((toks, width), BF16),
        in_specs=[hbm] * 9,
        out_specs=pl.BlockSpec(memory_space=pltpu.VMEM),
        scratch_shapes=[
            vmem((PAD, width), F32),
            vmem((rows, width), BF16),
            vmem((rows, 128), F32),
            vmem((toks, width), BF16),
            vmem((layers, width), F32),
            vmem((layers, width), F32),
            vmem((layers, width, HEAD_DIM), BF16),
            vmem((layers, width, HEAD_DIM), BF16),
            vmem((layers, width, HEAD_DIM), BF16),
            vmem((layers, HEAD_DIM, width), BF16),
            pltpu.SMEM((layers,), F32),
            vmem((rows, width), BF16),
            vmem((2, 4, rows, HEAD_DIM), BF16),
            vmem((2, ny, rows, HEAD_DIM), BF16),
            vmem((3, nz, PAD, HEAD_DIM), BF16),
            vmem((nz, PAD, HEAD_DIM), BF16),
            vmem((2, nz, PAD, HEAD_DIM), BF16),
            vmem((2, nz, PAD, HEAD_DIM), BF16),
            vmem((nz, PAD, HEAD_DIM), BF16),
            vmem((nz, PAD, HEAD_DIM), BF16),
            vmem((layers, nt, PAD, width), BF16),
            dma((13,)),
            dma((2, 4)),
            dma((2, 4)),
            dma((2, 2, half)),
            dma((2, ny)),
            dma((layers,)),
            dma((layers,)),
            dma((layers,)),
            dma((layers,)),
            dma((layers,)),
            dma((layers,)),
        ],
        compiler_params=pltpu.CompilerParams(collective_id=0, has_side_effects=True),
    )(*arrays)


SP = ("z", "y")


def torus_of(mesh):
    return Mesh(mesh.devices.reshape(16, 8, mesh.shape["tp"]), ("z", "y", "tp"))


def on_torus(torus):
    sizes = tuple(torus.shape[a] for a in ("z", "y", "tp"))
    return jax.shard_map(
        functools.partial(body, sizes),
        mesh=torus,
        in_specs=(
            P(SP, None),
            P(SP, None),
            P(),
            P(),
            P(None, None, "tp"),
            P(None, None, "tp"),
            P(None, None, "tp"),
            P(None, "tp", None),
            P(None, "tp"),
        ),
        out_specs=P(SP, None),
        check_vma=False,
    )


def solution(mesh):
    return on_torus(torus_of(mesh))
```

```python
import functools
import math

import jax
import jax.numpy as jnp
from jax import lax
from jax.experimental import pallas as pl
from jax.experimental.pallas import tpu as pltpu
from jax.sharding import Mesh
from jax.sharding import PartitionSpec as P

HEAD_DIM = 256
ROOT = math.sqrt(HEAD_DIM)
EPS = 1e-06
PAD = 8
MESH = pl.DeviceIdType.MESH
scope = jax.named_scope
BF16 = jnp.bfloat16
F32 = jnp.float32


def row_scale(values):
    return lax.rsqrt(jnp.mean(values * values, axis=-1, keepdims=True) + EPS)


def dot_nt(a, b):
    return lax.dot_general(a, b, (((1,), (1,)), ((), ())), preferred_element_type=F32)


def kernel(
    sizes,
    target,
    source,
    tgt_gain,
    src_gain,
    w_query,
    w_key,
    w_value,
    w_out,
    score_scale,
    out,
    hid,
    src,
    scale_of,
    tgt,
    tgain,
    sgain,
    wq,
    wk,
    wv,
    wo,
    scl,
    ns,
    kv0,
    kv1,
    q0,
    q1,
    nsend0,
    nrecv0,
    nsend1,
    nrecv1,
    share,
    halves,
    swap,
    load_sem,
    kv0_send,
    kv0_recv,
    kv1_send,
    kv1_recv,
    q_send,
    q_recv,
    h_send,
    h_recv,
    n0_send,
    n0_recv,
    n1_send,
    n1_recv,
    t_send,
    t_recv,
    s_send,
    s_recv,
):
    nz, ny, nt = sizes
    half = ny // 2
    z, y, t = lax.axis_index("z"), lax.axis_index("y"), lax.axis_index("tp")
    layers = wq.shape[0]
    rows = src.shape[0]
    toks = target.shape[0]
    mid = nz // 2
    groups = ((0, mid), (mid, nz))
    tall = mid * PAD
    width = hid.shape[2]

    def wrapped(i, n):
        return jnp.where(i >= n, i - n, i)

    def line(dy):
        return wrapped(y + (dy % ny), ny)

    def plane(k):
        return wrapped(z + k, nz)

    def other(k):
        return wrapped(t + k, nt)

    core = lax.rem(t, 2)
    partner = {"tp": t + 1 - 2 * core}

    def load(i, a, b):
        return pltpu.make_async_copy(a, b, load_sem.at[i])

    first = [
        load(0, target, tgt),
        load(1, tgt_gain, tgain),
        load(2, w_query.at[0], wq.at[0]),
        load(3, source, src),
        load(4, src_gain, sgain),
        load(5, w_key.at[0], wk.at[0]),
        load(6, w_value.at[0], wv.at[0]),
    ]
    later = [
        load(7, score_scale, scl),
        load(8, w_key.at[1], wk.at[1]),
        load(9, w_value.at[1], wv.at[1]),
        load(10, w_out.at[0], wo.at[0]),
        load(11, w_query.at[1], wq.at[1]),
        load(12, w_out.at[1], wo.at[1]),
    ]
    for one in first:
        one.start()

    barrier = pltpu.get_barrier_semaphore()

    def greet(peer):
        pl.semaphore_signal(barrier, inc=1, device_id=peer, device_id_type=MESH)

    sides = (2, -2)
    for dy in (1, -1) + sides:
        greet({"y": line(dy)})
    for k in range(1, nt):
        greet({"tp": other(k)})

    def far_first(i):
        away = (i + 1) // 2
        return wrapped(mid + jnp.where(lax.rem(i, 2) == 1, away, -away), nz)

    def greet_planes(i, carry):
        k = far_first(i)
        greet({"z": plane(k)})
        for dy in sides:
            greet({"z": plane(k), "y": line(dy)})
        return carry

    lax.fori_loop(0, nz - 1, greet_planes, 0)
    greeted = 4 + nt - 1 + (nz - 1) * 3
    for one in later:
        one.start()

    step = 16

    def at_rows(i):
        return pl.ds(pl.multiple_of(i * step, step), step)

    def both_layers(i, carry):
        for u in range(2):
            at = at_rows(2 * i + u)
            x = src[at, :].astype(F32)
            for layer in range(layers):
                ns[layer, at, :] = (x * sgain[layer : layer + 1, :]).astype(BF16)
            x = x * x
            total = x[:, 0:128]
            for c in range(128, x.shape[1], 128):
                total = total + x[:, c : c + 128]
            scale_of[at, :] = total
        return carry

    def source_scale():
        mean = jnp.sum(scale_of[...], axis=-1, keepdims=True) * (1.0 / src.shape[1])
        return lax.rsqrt(mean + EPS)

    def keys_of(layer):
        keys = jnp.dot(ns[layer], wk[layer], preferred_element_type=F32) * source_scale()
        return (keys * row_scale(keys)).astype(BF16)

    def values_of(layer):
        values = jnp.dot(ns[layer], wv[layer], preferred_element_type=F32) * source_scale()
        return values.astype(BF16)

    def queries_of(layer):
        hidden = jnp.concatenate([hid[0], hid[1]], axis=1)
        normed = (hidden * row_scale(hidden) * tgain[layer : layer + 1, :]).astype(BF16)
        queries = jnp.dot(normed, wq[layer], preferred_element_type=F32)
        return (queries * row_scale(queries)).astype(BF16)

    def push(src_ref, dst_ref, send, recv, peer):
        return pltpu.make_async_remote_copy(
            src_ref=src_ref,
            dst_ref=dst_ref,
            send_sem=send,
            recv_sem=recv,
            device_id=peer,
            device_id_type=MESH,
        )

    sign = 1 - 2 * lax.rem(t, 2)
    ahead, behind = lax.rem(y + sign + ny, ny), lax.rem(y - sign + ny, ny)

    def near(which, held, lands):
        return push(
            kv0.at[which, held],
            kv0.at[which, lands],
            kv0_send.at[which, lands],
            kv0_recv.at[which, lands],
            {"y": ahead if lands == 3 else behind},
        )

    right, left = line(1), line(-1)

    def ring(which, step):
        copies = []
        for way, peer in ((0, right), (1, left)):
            if step == half - 1 and which != way:
                continue
            held = 0 if step == 0 else (step if way == 0 else half + step)
            lands = half if step == half - 1 else (step + 1 if way == 0 else half + step + 1)
            copies.append(
                push(
                    kv1.at[which, held],
                    kv1.at[which, lands],
                    kv1_send.at[which, way, step],
                    kv1_recv.at[which, lands],
                    {"y": peer},
                )
            )
        return copies

    def ring_next(step):
        for which in (0, 1):
            for copy in ring(which, step):
                copy.wait_recv()
            if step < half - 1:
                for copy in ring(which, step + 1):
                    copy.start()

    def hop(d):
        return push(
            q0.at[2, 0],
            q0.at[d, z],
            h_send.at[0, d],
            h_recv.at[0, d],
            {"y": line(sides[d])},
        )

    def q0_straight():
        def go(i, carry):
            for d in range(2):
                push(
                    q0.at[2, 0],
                    q0.at[d, z],
                    q_send.at[0],
                    q_recv.at[0, 0],
                    {"z": plane(far_first(i)), "y": line(sides[d])},
                ).start()
            return carry

        lax.fori_loop(0, nz, go, 0)

    def q0_relay(d):
        def go(i, carry):
            push(
                q0.at[d, z],
                q0.at[d, z],
                q_send.at[0],
                q_recv.at[0, 1],
                {"z": plane(far_first(i))},
            ).start()
            return carry

        lax.fori_loop(0, nz - 1, go, 0)

    def n0_start(g):
        def go(i, carry):
            for d in range(2):
                push(
                    nsend0.at[d, i],
                    nrecv0.at[d, z],
                    n0_send,
                    n0_recv,
                    {"z": i, "y": line(-sides[d])},
                ).start()
            return carry

        lax.fori_loop(*groups[g], go, 0)

    early = z < mid

    def wait_group(layer, g, some_of):
        inside = early if g == 0 else jnp.logical_not(early)
        for less, when in ((1, inside), (0, jnp.logical_not(inside))):

            @pl.when(when)
            def _(less=less):
                some = some_of(mid - less)
                push(some, some, q_send.at[layer], q_recv.at[layer, g], {"z": plane(1)}).wait_recv()

    def q1_start():
        for g, (low, high) in enumerate(groups):

            def go(i, carry):
                @pl.when(i != z)
                def _():
                    push(
                        q1.at[nz], q1.at[z], q_send.at[1], q_recv.at[1, lax.div(z, mid)], {"z": i}
                    ).start()

                return carry

            lax.fori_loop(low, high, go, 0)

    def n1_start(g):
        def go(i, carry):
            @pl.when(i != z)
            def _():
                push(nsend1.at[i], nrecv1.at[z], n1_send, n1_recv, {"z": i}).start()

            return carry

        lax.fori_loop(*groups[g], go, 0)

    def share_start(layer):
        for k in sorted(range(1, nt), key=lambda k: abs(k - nt // 2)):
            push(
                share.at[layer, lax.rem(t + k, 2)],
                halves.at[layer, nt - k],
                t_send.at[layer],
                t_recv.at[layer],
                {"tp": other(k)},
            ).start()

    waits = []

    def wait_all(ref, send, recv, peer):
        both = push(ref, ref, send, recv, peer)
        both.wait_recv()
        waits.append(both)

    def weigh(layer, queries, keys):
        scores = dot_nt(queries, keys)
        weights = jnp.exp(scl[layer] * (scores * (1.0 / ROOT) - ROOT))
        sums = weights[:, 0:128]
        for c in range(128, weights.shape[1], 128):
            sums = sums + weights[:, c : c + 128]
        return weights.astype(BF16), sums

    def with_denominators(numer, sums):
        count = numer.shape[0]
        denoms = jnp.sum(sums.T, axis=0, keepdims=True)
        upper = denoms.astype(BF16).astype(F32)
        parts = [upper, denoms - upper]
        if count < 128:
            pad = jnp.zeros((1, 128 - count), F32)
            parts = [parts[0], pad, parts[1], pad]
        extra = jnp.concatenate(parts, axis=1).reshape(1, 1, 256)
        shape = (count // PAD, PAD, HEAD_DIM)
        lane = lax.rem(lax.broadcasted_iota(jnp.int32, shape, 2), 128)
        block = lax.broadcasted_iota(jnp.int32, shape, 0)
        row = lax.broadcasted_iota(jnp.int32, shape, 1)
        mine = jnp.where(lane // PAD == block, jnp.broadcast_to(extra, shape), 0.0)
        return jnp.where(row == PAD - 1, mine, numer.reshape(shape)).astype(BF16)

    def share_of(layer, total):
        shape = (PAD, 128)
        lane = lax.broadcasted_iota(jnp.int32, shape, 1)
        row = lax.broadcasted_iota(jnp.int32, shape, 0)
        both = total[PAD - 1 : PAD, 0:128] + total[PAD - 1 : PAD, 128:256]
        denoms = jnp.sum(
            jnp.where(lax.rem(lane, PAD) == row, jnp.broadcast_to(both, shape), 0.0),
            axis=1,
            keepdims=True,
        )
        real = lax.broadcasted_iota(jnp.int32, (PAD, HEAD_DIM), 0) < toks
        attended = jnp.where(real, total / denoms, 0.0).astype(BF16)
        rounded = jnp.dot(attended, wo[layer], preferred_element_type=F32).astype(BF16)
        share[layer, 0] = rounded[:, 0:width]
        share[layer, 1] = rounded[:, width : 2 * width]
        share_start(layer)

    def add_branch(layer):
        wait_all(halves.at[layer, pl.ds(1, nt - 1)], t_send.at[layer], t_recv.at[layer], partner)
        branch = share[layer, core].astype(F32)
        for k in range(1, nt):
            branch = branch + halves[layer, k].astype(F32)
        swap[layer, core] = (hid[core] + branch).astype(BF16)
        both = push(
            swap.at[layer, core], swap.at[layer, core], s_send.at[layer], s_recv.at[layer], partner
        )
        both.start()
        both.wait_recv()
        waits.append(both)

    with scope("queries_0"):
        for i in range(3):
            first[i].wait()
        hid[...] = jnp.zeros_like(hid)
        rows_in = tgt[...].astype(F32)
        hid[0, 0:toks, :] = rows_in[:, 0:width]
        hid[1, 0:toks, :] = rows_in[:, width : 2 * width]
        q0[2, 0] = queries_of(0)
    with scope("norm"):
        first[3].wait()
        first[4].wait()
        lax.fori_loop(0, rows // (2 * step), both_layers, 0)
    with scope("keys_0"):
        first[5].wait()
        kv0[0, 0] = keys_of(0)
    with scope("barrier"):
        pl.semaphore_wait(barrier, greeted)

    @pl.when(early)
    def _():
        q0_straight()

    @pl.when(jnp.logical_not(early))
    def _():
        for d in range(2):
            hop(d).start()

    near(0, 0, 1).start()
    near(0, 0, 3).start()
    with scope("values_0"):
        first[6].wait()
        kv0[1, 0] = values_of(0)
    near(1, 0, 1).start()
    near(1, 0, 3).start()
    with scope("source_1"):
        for i in (0, 1, 2):
            later[i].wait()
        kv1[0, 0] = keys_of(1)
        kv1[1, 0] = values_of(1)
        for i in (3, 4, 5):
            later[i].wait()
    with scope("hop_0"):

        @pl.when(jnp.logical_not(early))
        def _():
            for d in range(2):
                hop(d).wait_recv()
                q0_relay(d)

    for which in (0, 1):
        with scope(f"near_0_{which}"):
            near(which, 0, 1).wait_recv()
            near(which, 1, 2).start()
            near(which, 0, 3).wait_recv()
    for g, (low, high) in enumerate(groups):
        with scope(f"q_wait_0_{g}"):
            some = q0.at[pl.ds(0, 2), pl.ds(low, mid)]
            if g == 0:
                push(some, some, q_send.at[0], q_recv.at[0, 0], {"z": plane(1)}).wait_recv()
            else:
                wait_group(0, g, lambda count, low=low: q0.at[pl.ds(0, 2), pl.ds(low, count)])
        numer = jnp.zeros((2 * tall, HEAD_DIM), F32)
        total = jnp.zeros((2 * tall, 128), F32)
        queries = q0[0:2, low:high].reshape(2 * tall, HEAD_DIM)
        for slot in (0, 1, 3, 2):
            if slot == 2 and g == 0:
                for which in (0, 1):
                    with scope(f"near_1_{which}"):
                        near(which, 1, 2).wait_recv()
                        for copy in ring(which, 0):
                            copy.start()
            with scope(f"attend_0_{g}_{slot}"):
                weights, sums = weigh(0, queries, kv0[0, slot])
                total = total + sums
            numer = numer + jnp.dot(weights, kv0[1, slot], preferred_element_type=F32)
        with scope(f"partials_0_{g}"):
            nsend0[:, low:high] = with_denominators(numer, total).reshape(2, mid, PAD, HEAD_DIM)
            n0_start(g)
    with scope("ring_1_0"):
        ring_next(0)
    with scope("ring_late"):

        @pl.when(jnp.logical_not(early))
        def _():
            ring_next(1)
            ring_next(2)

    with scope("n_wait_0"):
        wait_all(nrecv0, n0_send, n0_recv, {"z": plane(1)})
    with scope("share_0"):
        share_of(0, jnp.sum(nrecv0[...].reshape(2 * nz, PAD, HEAD_DIM).astype(F32), axis=0))
    def serve(g):
        low, high = groups[g]
        with scope(f"q_wait_1_{g}"):
            wait_group(1, g, lambda count, low=low: q1.at[pl.ds(low, count)])
        with scope(f"attend_1_{g}"):
            numer = jnp.zeros((tall, HEAD_DIM), F32)
            total = jnp.zeros((tall, 128), F32)
            queries = q1[low:high].reshape(tall, HEAD_DIM)
            for slot in range(0, ny, 2):
                keys = kv1[0, slot : slot + 2].reshape(2 * rows, HEAD_DIM)
                weights, sums = weigh(1, queries, keys)
                total = total + sums
                values = kv1[1, slot : slot + 2].reshape(2 * rows, HEAD_DIM)
                numer = numer + jnp.dot(weights, values, preferred_element_type=F32)
        with scope(f"partials_1_{g}"):
            nsend1[low:high] = with_denominators(numer, total)
            n1_start(g)

    @pl.when(early)
    def _():
        with scope("ring_1_1"):
            ring_next(1)

    @pl.when(jnp.logical_not(early))
    def _():
        with scope("ring_1_3"):
            ring_next(3)
        serve(0)

    with scope("t_wait_0"):
        add_branch(0)
    with scope("queries_1"):
        hid[...] = swap[0].astype(F32)
        own = queries_of(1)
        q1[nz] = own
        q1[z] = own
        q1_start()
    @pl.when(early)
    def _():
        with scope("ring_early"):
            ring_next(2)
            ring_next(3)
        serve(0)

    @pl.when(jnp.logical_not(early))
    def _():
        serve(1)

    with scope("n_wait_1"):
        nrecv1[z] = nsend1[z]
        some = nrecv1.at[pl.ds(0, nz - 1)]
        wait_all(some, n1_send, n1_recv, {"z": plane(1)})
    with scope("share_1"):
        share_of(1, jnp.sum(nrecv1[...].astype(F32), axis=0))

    @pl.when(early)
    def _():
        serve(1)

    with scope("t_wait_1"):
        add_branch(1)
    with scope("drain"):
        out[:, 0:width] = swap[1, 0][0:toks, :]
        out[:, width : 2 * width] = swap[1, 1][0:toks, :]
        for both in waits:
            both.wait_send()

        def sent(layer, some):
            push(
                some, some, q_send.at[layer], q_recv.at[layer, 0], {"z": plane(1)}
            ).wait_send()

        sent(1, q1.at[pl.ds(0, nz - 1)])

        @pl.when(early)
        def _():
            sent(0, q0.at[pl.ds(0, 2)])

        @pl.when(jnp.logical_not(early))
        def _():
            sent(0, q0.at[pl.ds(0, 2), pl.ds(0, nz - 1)])
            for d in range(2):
                hop(d).wait_send()

        for which in (0, 1):
            for held, lands in ((0, 1), (0, 3), (1, 2)):
                near(which, held, lands).wait_send()
            for s in range(half):
                for copy in ring(which, s):
                    copy.wait_send()


def body(sizes, *arrays):
    target, source = arrays[0], arrays[1]
    w_query = arrays[4]
    arrays = (*arrays[:8], arrays[8].reshape(-1))
    nz, ny, nt = sizes
    toks, width = target.shape
    rows = source.shape[0]
    layers = w_query.shape[0]
    half = ny // 2
    hbm = pl.BlockSpec(memory_space=pl.ANY)
    vmem = pltpu.VMEM
    dma = pltpu.SemaphoreType.DMA
    return pl.pallas_call(
        functools.partial(kernel, sizes),
        out_shape=pltpu.VMEM((toks, width), BF16),
        in_specs=[hbm] * 9,
        out_specs=pl.BlockSpec(memory_space=pltpu.VMEM),
        scratch_shapes=[
            vmem((2, PAD, width // 2), F32),
            vmem((rows, width), BF16),
            vmem((rows, 128), F32),
            vmem((toks, width), BF16),
            vmem((layers, width), F32),
            vmem((layers, width), F32),
            vmem((layers, width, HEAD_DIM), BF16),
            vmem((layers, width, HEAD_DIM), BF16),
            vmem((layers, width, HEAD_DIM), BF16),
            vmem((layers, HEAD_DIM, width), BF16),
            pltpu.SMEM((layers,), F32),
            vmem((layers, rows, width), BF16),
            vmem((2, 4, rows, HEAD_DIM), BF16),
            vmem((2, ny, rows, HEAD_DIM), BF16),
            vmem((3, nz, PAD, HEAD_DIM), BF16),
            vmem((nz + 1, PAD, HEAD_DIM), BF16),
            vmem((2, nz, PAD, HEAD_DIM), BF16),
            vmem((2, nz, PAD, HEAD_DIM), BF16),
            vmem((nz, PAD, HEAD_DIM), BF16),
            vmem((nz, PAD, HEAD_DIM), BF16),
            vmem((layers, 2, PAD, width // 2), BF16),
            vmem((layers, nt, PAD, width // 2), BF16),
            vmem((layers, 2, PAD, width // 2), BF16),
            dma((13,)),
            dma((2, 4)),
            dma((2, 4)),
            dma((2, 2, half)),
            dma((2, ny)),
            dma((layers,)),
            dma((layers, 2)),
            dma((1, 2)),
            dma((1, 2)),
            dma,
            dma,
            dma,
            dma,
            dma((layers,)),
            dma((layers,)),
            dma((layers,)),
            dma((layers,)),
        ],
        compiler_params=pltpu.CompilerParams(collective_id=0, has_side_effects=True),
    )(*arrays)


SP = ("z", "y")


def torus_of(mesh):
    return Mesh(mesh.devices.reshape(16, 8, mesh.shape["tp"]), ("z", "y", "tp"))


def on_torus(torus):
    sizes = tuple(torus.shape[a] for a in ("z", "y", "tp"))
    return jax.shard_map(
        functools.partial(body, sizes),
        mesh=torus,
        in_specs=(
            P(SP, None),
            P(SP, None),
            P(),
            P(),
            P(None, None, "tp"),
            P(None, None, "tp"),
            P(None, None, "tp"),
            P(None, "tp", None),
            P(None, "tp"),
        ),
        out_specs=P(SP, None),
        check_vma=False,
    )


def solution(mesh):
    return on_torus(torus_of(mesh))
```

```python
import functools
import math

import jax
import jax.numpy as jnp
from jax import lax
from jax.experimental import pallas as pl
from jax.experimental.pallas import tpu as pltpu
from jax.sharding import Mesh
from jax.sharding import PartitionSpec as P

HEAD_DIM = 256
ROOT = math.sqrt(HEAD_DIM)
EPS = 1e-06
PAD = 8
MESH = pl.DeviceIdType.MESH
scope = jax.named_scope
BF16 = jnp.bfloat16
F32 = jnp.float32


def row_scale(values):
    return lax.rsqrt(jnp.mean(values * values, axis=-1, keepdims=True) + EPS)


def dot_nt(a, b):
    return lax.dot_general(a, b, (((1,), (1,)), ((), ())), preferred_element_type=F32)


def kernel(
    sizes,
    target,
    source,
    tgt_gain,
    src_gain,
    w_query,
    w_key,
    w_value,
    w_out,
    score_scale,
    out,
    hid,
    src,
    scale_of,
    tgt,
    tgain,
    sgain,
    wq,
    wk,
    wv,
    wo,
    scl,
    ns,
    kv0,
    kv1,
    q0,
    q1,
    nsend0,
    nrecv0,
    nsend1,
    nrecv1,
    share,
    back_send,
    back_recv,
    gathered,
    halves,
    swap,
    load_sem,
    kv0_send,
    kv0_recv,
    kv1_send,
    kv1_recv,
    q_send,
    q_recv,
    h_send,
    h_recv,
    b_send,
    b_recv,
    n0_send,
    n0_recv,
    n1_send,
    n1_recv,
    t_send,
    t_recv,
    s_send,
    s_recv,
):
    nz, ny, nt = sizes
    half = ny // 2
    z, y, t = lax.axis_index("z"), lax.axis_index("y"), lax.axis_index("tp")
    layers = wq.shape[0]
    rows = src.shape[0]
    toks = target.shape[0]
    mid = nz // 2
    groups = ((0, mid), (mid, nz))
    tall = mid * PAD
    width = hid.shape[2]

    def wrapped(i, n):
        return jnp.where(i >= n, i - n, i)

    def line(dy):
        return wrapped(y + (dy % ny), ny)

    def plane(k):
        return wrapped(z + k, nz)

    def other(k):
        return wrapped(t + k, nt)

    core = lax.rem(t, 2)
    partner = {"tp": t + 1 - 2 * core}

    def load(i, a, b):
        return pltpu.make_async_copy(a, b, load_sem.at[i])

    first = [
        load(0, target, tgt),
        load(1, tgt_gain, tgain),
        load(2, w_query.at[0], wq.at[0]),
        load(3, source, src),
        load(4, src_gain, sgain),
        load(5, w_key.at[0], wk.at[0]),
        load(6, w_value.at[0], wv.at[0]),
    ]
    later = [
        load(7, score_scale, scl),
        load(8, w_key.at[1], wk.at[1]),
        load(9, w_value.at[1], wv.at[1]),
        load(10, w_out.at[0], wo.at[0]),
        load(11, w_query.at[1], wq.at[1]),
        load(12, w_out.at[1], wo.at[1]),
    ]
    for one in first:
        one.start()

    barrier = pltpu.get_barrier_semaphore()

    def greet(peer):
        pl.semaphore_signal(barrier, inc=1, device_id=peer, device_id_type=MESH)

    sides = (2, -2)
    for dy in (1, -1) + sides:
        greet({"y": line(dy)})
    for k in range(1, nt):
        greet({"tp": other(k)})

    def far_first(i):
        away = (i + 1) // 2
        return wrapped(mid + jnp.where(lax.rem(i, 2) == 1, away, -away), nz)

    def greet_planes(i, carry):
        k = far_first(i)
        greet({"z": plane(k)})
        for dy in sides:
            greet({"z": plane(k), "y": line(dy)})
        return carry

    lax.fori_loop(0, nz - 1, greet_planes, 0)
    greeted = 4 + nt - 1 + (nz - 1) * 3
    for one in later:
        one.start()

    step = 16

    def at_rows(i):
        return pl.ds(pl.multiple_of(i * step, step), step)

    def both_layers(i, carry):
        for u in range(2):
            at = at_rows(2 * i + u)
            x = src[at, :].astype(F32)
            for layer in range(layers):
                ns[layer, at, :] = (x * sgain[layer : layer + 1, :]).astype(BF16)
            x = x * x
            total = x[:, 0:128]
            for c in range(128, x.shape[1], 128):
                total = total + x[:, c : c + 128]
            scale_of[at, :] = total
        return carry

    def source_scale():
        mean = jnp.sum(scale_of[...], axis=-1, keepdims=True) * (1.0 / src.shape[1])
        return lax.rsqrt(mean + EPS)

    def keys_of(layer):
        keys = jnp.dot(ns[layer], wk[layer], preferred_element_type=F32) * source_scale()
        return (keys * row_scale(keys)).astype(BF16)

    def values_of(layer):
        values = jnp.dot(ns[layer], wv[layer], preferred_element_type=F32) * source_scale()
        return values.astype(BF16)

    def queries_of(layer):
        hidden = jnp.concatenate([hid[0], hid[1]], axis=1)
        normed = (hidden * row_scale(hidden) * tgain[layer : layer + 1, :]).astype(BF16)
        queries = jnp.dot(normed, wq[layer], preferred_element_type=F32)
        return (queries * row_scale(queries)).astype(BF16)

    def push(src_ref, dst_ref, send, recv, peer):
        return pltpu.make_async_remote_copy(
            src_ref=src_ref,
            dst_ref=dst_ref,
            send_sem=send,
            recv_sem=recv,
            device_id=peer,
            device_id_type=MESH,
        )

    sign = 1 - 2 * lax.rem(t, 2)
    ahead, behind = lax.rem(y + sign + ny, ny), lax.rem(y - sign + ny, ny)

    def near(which, held, lands):
        return push(
            kv0.at[which, held],
            kv0.at[which, lands],
            kv0_send.at[which, lands],
            kv0_recv.at[which, lands],
            {"y": ahead if lands == 3 else behind},
        )

    right, left = line(1), line(-1)

    def ring(which, step):
        copies = []
        for way, peer in ((0, right), (1, left)):
            if step == half - 1 and which != way:
                continue
            held = 0 if step == 0 else (step if way == 0 else half + step)
            lands = half if step == half - 1 else (step + 1 if way == 0 else half + step + 1)
            copies.append(
                push(
                    kv1.at[which, held],
                    kv1.at[which, lands],
                    kv1_send.at[which, way, step],
                    kv1_recv.at[which, lands],
                    {"y": peer},
                )
            )
        return copies

    def ring_next(step):
        for which in (0, 1):
            for copy in ring(which, step):
                copy.wait_recv()
            if step < half - 1:
                for copy in ring(which, step + 1):
                    copy.start()

    def hop(d):
        return push(
            q0.at[2, 0],
            q0.at[d, z],
            h_send.at[0, d],
            h_recv.at[0, d],
            {"y": line(sides[d])},
        )

    def q0_straight():
        def go(i, carry):
            for d in range(2):
                push(
                    q0.at[2, 0],
                    q0.at[d, z],
                    q_send.at[0],
                    q_recv.at[0, 0],
                    {"z": plane(far_first(i)), "y": line(sides[d])},
                ).start()
            return carry

        lax.fori_loop(0, nz, go, 0)

    def q0_relay(d):
        def go(i, carry):
            push(
                q0.at[d, z],
                q0.at[d, z],
                q_send.at[0],
                q_recv.at[0, 1],
                {"z": plane(far_first(i))},
            ).start()
            return carry

        lax.fori_loop(0, nz - 1, go, 0)

    def n0_straight():
        def go(i, carry):
            for d in range(2):
                push(
                    nsend0.at[d, i],
                    nrecv0.at[d, z],
                    n0_send,
                    n0_recv,
                    {"z": i, "y": line(-sides[d])},
                ).start()
            return carry

        lax.fori_loop(*groups[0], go, 0)

    def n0_along():
        def go(i, carry):
            @pl.when(i != z)
            def _():
                for d in range(2):
                    push(
                        nsend0.at[d, i], nrecv0.at[d, z], n0_send, n0_recv, {"z": i}
                    ).start()

            return carry

        lax.fori_loop(*groups[1], go, 0)

    def back(d):
        return push(
            back_send.at[d],
            back_recv.at[d],
            b_send.at[d],
            b_recv.at[d],
            {"y": line(-sides[d])},
        )

    early = z < mid

    def wait_group(layer, g, some_of):
        inside = early if g == 0 else jnp.logical_not(early)
        for less, when in ((1, inside), (0, jnp.logical_not(inside))):

            @pl.when(when)
            def _(less=less):
                some = some_of(mid - less)
                push(some, some, q_send.at[layer], q_recv.at[layer, g], {"z": plane(1)}).wait_recv()

    def q1_start():
        for g, (low, high) in enumerate(groups):

            def go(i, carry):
                @pl.when(i != z)
                def _():
                    push(
                        q1.at[nz], q1.at[z], q_send.at[1], q_recv.at[1, lax.div(z, mid)], {"z": i}
                    ).start()

                return carry

            lax.fori_loop(low, high, go, 0)

    def n1_start(g):
        def go(i, carry):
            @pl.when(i != z)
            def _():
                push(nsend1.at[i], nrecv1.at[z], n1_send, n1_recv, {"z": i}).start()

            return carry

        lax.fori_loop(*groups[g], go, 0)

    def share_start(layer):
        for k in sorted(range(1, nt), key=lambda k: abs(k - nt // 2)):
            push(
                share.at[layer, lax.rem(t + k, 2)],
                halves.at[layer, nt - k],
                t_send.at[layer],
                t_recv.at[layer],
                {"tp": other(k)},
            ).start()

    waits = []

    def wait_all(ref, send, recv, peer):
        both = push(ref, ref, send, recv, peer)
        both.wait_recv()
        waits.append(both)

    def weigh(layer, queries, keys):
        scores = dot_nt(queries, keys)
        weights = jnp.exp(scl[layer] * (scores * (1.0 / ROOT) - ROOT))
        sums = weights[:, 0:128]
        for c in range(128, weights.shape[1], 128):
            sums = sums + weights[:, c : c + 128]
        return weights.astype(BF16), sums

    def with_denominators(numer, sums):
        count = numer.shape[0]
        denoms = jnp.sum(sums.T, axis=0, keepdims=True)
        upper = denoms.astype(BF16).astype(F32)
        parts = [upper, denoms - upper]
        if count < 128:
            pad = jnp.zeros((1, 128 - count), F32)
            parts = [parts[0], pad, parts[1], pad]
        extra = jnp.concatenate(parts, axis=1).reshape(1, 1, 256)
        shape = (count // PAD, PAD, HEAD_DIM)
        lane = lax.rem(lax.broadcasted_iota(jnp.int32, shape, 2), 128)
        block = lax.broadcasted_iota(jnp.int32, shape, 0)
        row = lax.broadcasted_iota(jnp.int32, shape, 1)
        mine = jnp.where(lane // PAD == block, jnp.broadcast_to(extra, shape), 0.0)
        return jnp.where(row == PAD - 1, mine, numer.reshape(shape)).astype(BF16)

    def share_of(layer, total):
        shape = (PAD, 128)
        lane = lax.broadcasted_iota(jnp.int32, shape, 1)
        row = lax.broadcasted_iota(jnp.int32, shape, 0)
        both = total[PAD - 1 : PAD, 0:128] + total[PAD - 1 : PAD, 128:256]
        denoms = jnp.sum(
            jnp.where(lax.rem(lane, PAD) == row, jnp.broadcast_to(both, shape), 0.0),
            axis=1,
            keepdims=True,
        )
        real = lax.broadcasted_iota(jnp.int32, (PAD, HEAD_DIM), 0) < toks
        attended = jnp.where(real, total / denoms, 0.0).astype(BF16)
        rounded = jnp.dot(attended, wo[layer], preferred_element_type=F32).astype(BF16)
        share[layer, 0] = rounded[:, 0:width]
        share[layer, 1] = rounded[:, width : 2 * width]
        share_start(layer)

    def add_branch(layer):
        wait_all(halves.at[layer, pl.ds(1, nt - 1)], t_send.at[layer], t_recv.at[layer], partner)
        branch = share[layer, core].astype(F32)
        for k in range(1, nt):
            branch = branch + halves[layer, k].astype(F32)
        swap[layer, core] = (hid[core] + branch).astype(BF16)
        both = push(
            swap.at[layer, core], swap.at[layer, core], s_send.at[layer], s_recv.at[layer], partner
        )
        both.start()
        both.wait_recv()
        waits.append(both)

    with scope("queries_0"):
        for i in range(3):
            first[i].wait()
        hid[...] = jnp.zeros_like(hid)
        rows_in = tgt[...].astype(F32)
        hid[0, 0:toks, :] = rows_in[:, 0:width]
        hid[1, 0:toks, :] = rows_in[:, width : 2 * width]
        q0[2, 0] = queries_of(0)
    with scope("norm"):
        first[3].wait()
        first[4].wait()
        lax.fori_loop(0, rows // (2 * step), both_layers, 0)
    with scope("keys_0"):
        first[5].wait()
        kv0[0, 0] = keys_of(0)
    with scope("barrier"):
        pl.semaphore_wait(barrier, greeted)

    @pl.when(early)
    def _():
        q0_straight()

    @pl.when(jnp.logical_not(early))
    def _():
        for d in range(2):
            hop(d).start()

    near(0, 0, 1).start()
    near(0, 0, 3).start()
    with scope("values_0"):
        first[6].wait()
        kv0[1, 0] = values_of(0)
    near(1, 0, 1).start()
    near(1, 0, 3).start()
    with scope("source_1"):
        for i in (0, 1, 2):
            later[i].wait()
        kv1[0, 0] = keys_of(1)
        kv1[1, 0] = values_of(1)
        for i in (3, 4, 5):
            later[i].wait()
    with scope("hop_0"):

        @pl.when(jnp.logical_not(early))
        def _():
            for d in range(2):
                hop(d).wait_recv()
                q0_relay(d)

    for which in (0, 1):
        with scope(f"near_0_{which}"):
            near(which, 0, 1).wait_recv()
            near(which, 1, 2).start()
            near(which, 0, 3).wait_recv()
    for g, (low, high) in enumerate(groups):
        with scope(f"q_wait_0_{g}"):
            some = q0.at[pl.ds(0, 2), pl.ds(low, mid)]
            if g == 0:
                push(some, some, q_send.at[0], q_recv.at[0, 0], {"z": plane(1)}).wait_recv()
            else:
                wait_group(0, g, lambda count, low=low: q0.at[pl.ds(0, 2), pl.ds(low, count)])
        numer = jnp.zeros((2 * tall, HEAD_DIM), F32)
        total = jnp.zeros((2 * tall, 128), F32)
        queries = q0[0:2, low:high].reshape(2 * tall, HEAD_DIM)
        for slot in (0, 1, 3, 2):
            if slot == 2 and g == 0:
                for which in (0, 1):
                    with scope(f"near_1_{which}"):
                        near(which, 1, 2).wait_recv()
                        for copy in ring(which, 0):
                            copy.start()
            with scope(f"attend_0_{g}_{slot}"):
                weights, sums = weigh(0, queries, kv0[0, slot])
                total = total + sums
            numer = numer + jnp.dot(weights, kv0[1, slot], preferred_element_type=F32)
        with scope(f"partials_0_{g}"):
            nsend0[:, low:high] = with_denominators(numer, total).reshape(2, mid, PAD, HEAD_DIM)
            n0_straight() if g == 0 else n0_along()
    with scope("ring_1_0"):
        ring_next(0)
    with scope("ring_late"):

        @pl.when(jnp.logical_not(early))
        def _():
            some = nrecv0.at[pl.ds(0, 2), pl.ds(0, nz - 1)]
            push(some, some, n0_send, n0_recv, {"z": plane(1)}).wait_recv()
            for d in range(2):
                nrecv0[d, z] = nsend0[d, z]
                back_send[d] = jnp.sum(nrecv0[d].astype(F32), axis=0)
                back(d).start()
            ring_next(1)
            for d in range(2):
                back(d).wait_recv()
            gathered[...] = back_recv[0] + back_recv[1]

    with scope("n_wait_0"):

        @pl.when(early)
        def _():
            push(nrecv0, nrecv0, n0_send, n0_recv, {"z": plane(1)}).wait_recv()
            gathered[...] = jnp.sum(
                nrecv0[...].reshape(2 * nz, PAD, HEAD_DIM).astype(F32), axis=0
            )

    with scope("share_0"):
        share_of(0, gathered[...])
    def serve(g):
        low, high = groups[g]
        with scope(f"q_wait_1_{g}"):
            wait_group(1, g, lambda count, low=low: q1.at[pl.ds(low, count)])
        with scope(f"attend_1_{g}"):
            numer = jnp.zeros((tall, HEAD_DIM), F32)
            total = jnp.zeros((tall, 128), F32)
            queries = q1[low:high].reshape(tall, HEAD_DIM)
            for slot in range(0, ny, 2):
                keys = kv1[0, slot : slot + 2].reshape(2 * rows, HEAD_DIM)
                weights, sums = weigh(1, queries, keys)
                total = total + sums
                values = kv1[1, slot : slot + 2].reshape(2 * rows, HEAD_DIM)
                numer = numer + jnp.dot(weights, values, preferred_element_type=F32)
        with scope(f"partials_1_{g}"):
            nsend1[low:high] = with_denominators(numer, total)
            n1_start(g)

    @pl.when(early)
    def _():
        with scope("ring_1_1"):
            ring_next(1)

    @pl.when(jnp.logical_not(early))
    def _():
        with scope("ring_1_2"):
            ring_next(2)

    with scope("t_wait_0"):
        add_branch(0)
    with scope("queries_1"):
        hid[...] = swap[0].astype(F32)
        own = queries_of(1)
        q1[nz] = own
        q1[z] = own
        q1_start()
    @pl.when(early)
    def _():
        ring_next(2)

    with scope("ring_1_3"):
        ring_next(3)
    serve(0)
    serve(1)
    with scope("n_wait_1"):
        nrecv1[z] = nsend1[z]
        some = nrecv1.at[pl.ds(0, nz - 1)]
        wait_all(some, n1_send, n1_recv, {"z": plane(1)})
    with scope("share_1"):
        share_of(1, jnp.sum(nrecv1[...].astype(F32), axis=0))
    with scope("t_wait_1"):
        add_branch(1)
    with scope("drain"):
        out[:, 0:width] = swap[1, 0][0:toks, :]
        out[:, width : 2 * width] = swap[1, 1][0:toks, :]
        for both in waits:
            both.wait_send()

        def sent(layer, some):
            push(
                some, some, q_send.at[layer], q_recv.at[layer, 0], {"z": plane(1)}
            ).wait_send()

        sent(1, q1.at[pl.ds(0, nz - 1)])

        @pl.when(early)
        def _():
            sent(0, q0.at[pl.ds(0, 2)])
            push(nrecv0, nrecv0, n0_send, n0_recv, {"z": plane(1)}).wait_send()

        @pl.when(jnp.logical_not(early))
        def _():
            sent(0, q0.at[pl.ds(0, 2), pl.ds(0, nz - 1)])
            for d in range(2):
                hop(d).wait_send()
                back(d).wait_send()
            some = nsend0.at[pl.ds(0, 2), pl.ds(0, nz - 1)]
            push(some, some, n0_send, n0_recv, {"z": plane(1)}).wait_send()

        for which in (0, 1):
            for held, lands in ((0, 1), (0, 3), (1, 2)):
                near(which, held, lands).wait_send()
            for s in range(half):
                for copy in ring(which, s):
                    copy.wait_send()


def body(sizes, *arrays):
    target, source = arrays[0], arrays[1]
    w_query = arrays[4]
    arrays = (*arrays[:8], arrays[8].reshape(-1))
    nz, ny, nt = sizes
    toks, width = target.shape
    rows = source.shape[0]
    layers = w_query.shape[0]
    half = ny // 2
    hbm = pl.BlockSpec(memory_space=pl.ANY)
    vmem = pltpu.VMEM
    dma = pltpu.SemaphoreType.DMA
    return pl.pallas_call(
        functools.partial(kernel, sizes),
        out_shape=pltpu.VMEM((toks, width), BF16),
        in_specs=[hbm] * 9,
        out_specs=pl.BlockSpec(memory_space=pltpu.VMEM),
        scratch_shapes=[
            vmem((2, PAD, width // 2), F32),
            vmem((rows, width), BF16),
            vmem((rows, 128), F32),
            vmem((toks, width), BF16),
            vmem((layers, width), F32),
            vmem((layers, width), F32),
            vmem((layers, width, HEAD_DIM), BF16),
            vmem((layers, width, HEAD_DIM), BF16),
            vmem((layers, width, HEAD_DIM), BF16),
            vmem((layers, HEAD_DIM, width), BF16),
            pltpu.SMEM((layers,), F32),
            vmem((layers, rows, width), BF16),
            vmem((2, 4, rows, HEAD_DIM), BF16),
            vmem((2, ny, rows, HEAD_DIM), BF16),
            vmem((3, nz, PAD, HEAD_DIM), BF16),
            vmem((nz + 1, PAD, HEAD_DIM), BF16),
            vmem((2, nz, PAD, HEAD_DIM), BF16),
            vmem((2, nz, PAD, HEAD_DIM), BF16),
            vmem((nz, PAD, HEAD_DIM), BF16),
            vmem((nz, PAD, HEAD_DIM), BF16),
            vmem((layers, 2, PAD, width // 2), BF16),
            vmem((2, PAD, HEAD_DIM), F32),
            vmem((2, PAD, HEAD_DIM), F32),
            vmem((PAD, HEAD_DIM), F32),
            vmem((layers, nt, PAD, width // 2), BF16),
            vmem((layers, 2, PAD, width // 2), BF16),
            dma((13,)),
            dma((2, 4)),
            dma((2, 4)),
            dma((2, 2, half)),
            dma((2, ny)),
            dma((layers,)),
            dma((layers, 2)),
            dma((1, 2)),
            dma((1, 2)),
            dma((2,)),
            dma((2,)),
            dma,
            dma,
            dma,
            dma,
            dma((layers,)),
            dma((layers,)),
            dma((layers,)),
            dma((layers,)),
        ],
        compiler_params=pltpu.CompilerParams(collective_id=0, has_side_effects=True),
    )(*arrays)


SP = ("z", "y")


def torus_of(mesh):
    return Mesh(mesh.devices.reshape(16, 8, mesh.shape["tp"]), ("z", "y", "tp"))


def on_torus(torus):
    sizes = tuple(torus.shape[a] for a in ("z", "y", "tp"))
    return jax.shard_map(
        functools.partial(body, sizes),
        mesh=torus,
        in_specs=(
            P(SP, None),
            P(SP, None),
            P(),
            P(),
            P(None, None, "tp"),
            P(None, None, "tp"),
            P(None, None, "tp"),
            P(None, "tp", None),
            P(None, "tp"),
        ),
        out_specs=P(SP, None),
        check_vma=False,
    )


def solution(mesh):
    return on_torus(torus_of(mesh))
```

```python
import functools
import math

import jax
import jax.numpy as jnp
from jax import lax
from jax.experimental import pallas as pl
from jax.experimental.pallas import tpu as pltpu
from jax.sharding import Mesh
from jax.sharding import PartitionSpec as P

HEAD_DIM = 256
ROOT = math.sqrt(HEAD_DIM)
EPS = 1e-06
PAD = 8
MESH = pl.DeviceIdType.MESH
scope = jax.named_scope
BF16 = jnp.bfloat16
F32 = jnp.float32


def row_scale(values):
    return lax.rsqrt(jnp.mean(values * values, axis=-1, keepdims=True) + EPS)


def dot_nt(a, b):
    return lax.dot_general(a, b, (((1,), (1,)), ((), ())), preferred_element_type=F32)


def kernel(
    sizes,
    target,
    source,
    tgt_gain,
    src_gain,
    w_query,
    w_key,
    w_value,
    w_out,
    score_scale,
    out,
    hid,
    src,
    scale_of,
    tgt,
    tgain,
    sgain,
    wq,
    wk,
    wv,
    wo,
    scl,
    ns,
    kv0,
    kv1,
    q0,
    q1,
    nsend0,
    nrecv0,
    nsend1,
    nrecv1,
    share,
    back_send,
    back_recv,
    gathered,
    halves,
    swap,
    load_sem,
    kv0_send,
    kv0_recv,
    kv1_send,
    kv1_recv,
    q_send,
    q_recv,
    h_send,
    h_recv,
    b_send,
    b_recv,
    n0_send,
    n0_recv,
    n1_send,
    n1_recv,
    t_send,
    t_recv,
    s_send,
    s_recv,
):
    nz, ny, nt = sizes
    half = ny // 2
    z, y, t = lax.axis_index("z"), lax.axis_index("y"), lax.axis_index("tp")
    layers = wq.shape[0]
    rows = src.shape[0]
    toks = target.shape[0]
    mid = nz // 2
    groups = ((0, mid), (mid, nz))
    tall = mid * PAD
    width = hid.shape[2]

    def wrapped(i, n):
        return jnp.where(i >= n, i - n, i)

    def line(dy):
        return wrapped(y + (dy % ny), ny)

    def plane(k):
        return wrapped(z + k, nz)

    def other(k):
        return wrapped(t + k, nt)

    core = lax.rem(t, 2)
    partner = {"tp": t + 1 - 2 * core}

    def load(i, a, b):
        return pltpu.make_async_copy(a, b, load_sem.at[i])

    first = [
        load(0, target, tgt),
        load(1, tgt_gain, tgain),
        load(2, w_query.at[0], wq.at[0]),
        load(3, source, src),
        load(4, src_gain, sgain),
        load(5, w_key.at[0], wk.at[0]),
        load(6, w_value.at[0], wv.at[0]),
    ]
    later = [
        load(7, score_scale, scl),
        load(8, w_key.at[1], wk.at[1]),
        load(9, w_value.at[1], wv.at[1]),
        load(10, w_out.at[0], wo.at[0]),
        load(11, w_query.at[1], wq.at[1]),
        load(12, w_out.at[1], wo.at[1]),
    ]
    for one in first:
        one.start()

    barrier = pltpu.get_barrier_semaphore()

    def greet(peer):
        pl.semaphore_signal(barrier, inc=1, device_id=peer, device_id_type=MESH)

    sides = (2, -2)
    for dy in (1, -1) + sides:
        greet({"y": line(dy)})
    for k in range(1, nt):
        greet({"tp": other(k)})

    def far_first(i):
        away = (i + 1) // 2
        return wrapped(mid + jnp.where(lax.rem(i, 2) == 1, away, -away), nz)

    def greet_planes(i, carry):
        k = far_first(i)
        greet({"z": plane(k)})
        for dy in sides:
            greet({"z": plane(k), "y": line(dy)})
        return carry

    lax.fori_loop(0, nz - 1, greet_planes, 0)
    greeted = 4 + nt - 1 + (nz - 1) * 3
    for one in later:
        one.start()

    step = 16

    def at_rows(i):
        return pl.ds(pl.multiple_of(i * step, step), step)

    def both_layers(i, carry):
        for u in range(2):
            at = at_rows(2 * i + u)
            x = src[at, :].astype(F32)
            for layer in range(layers):
                ns[layer, at, :] = (x * sgain[layer : layer + 1, :]).astype(BF16)
            x = x * x
            total = x[:, 0:128]
            for c in range(128, x.shape[1], 128):
                total = total + x[:, c : c + 128]
            scale_of[at, :] = total
        return carry

    def source_scale():
        mean = jnp.sum(scale_of[...], axis=-1, keepdims=True) * (1.0 / src.shape[1])
        return lax.rsqrt(mean + EPS)

    def keys_of(layer):
        keys = jnp.dot(ns[layer], wk[layer], preferred_element_type=F32) * source_scale()
        return (keys * row_scale(keys)).astype(BF16)

    def values_of(layer):
        values = jnp.dot(ns[layer], wv[layer], preferred_element_type=F32) * source_scale()
        return values.astype(BF16)

    def queries_of(layer):
        hidden = jnp.concatenate([hid[0], hid[1]], axis=1)
        normed = (hidden * row_scale(hidden) * tgain[layer : layer + 1, :]).astype(BF16)
        queries = jnp.dot(normed, wq[layer], preferred_element_type=F32)
        return (queries * row_scale(queries)).astype(BF16)

    def push(src_ref, dst_ref, send, recv, peer):
        return pltpu.make_async_remote_copy(
            src_ref=src_ref,
            dst_ref=dst_ref,
            send_sem=send,
            recv_sem=recv,
            device_id=peer,
            device_id_type=MESH,
        )

    sign = 1 - 2 * lax.rem(t, 2)
    ahead, behind = lax.rem(y + sign + ny, ny), lax.rem(y - sign + ny, ny)

    def near(which, held, lands):
        return push(
            kv0.at[which, held],
            kv0.at[which, lands],
            kv0_send.at[which, lands],
            kv0_recv.at[which, lands],
            {"y": ahead if lands == 3 else behind},
        )

    right, left = line(1), line(-1)

    def ring(which, step):
        copies = []
        for way, peer in ((0, right), (1, left)):
            if step == half - 1 and which != way:
                continue
            held = 0 if step == 0 else (step if way == 0 else half + step)
            lands = half if step == half - 1 else (step + 1 if way == 0 else half + step + 1)
            copies.append(
                push(
                    kv1.at[which, held],
                    kv1.at[which, lands],
                    kv1_send.at[which, way, step],
                    kv1_recv.at[which, lands],
                    {"y": peer},
                )
            )
        return copies

    def ring_next(step):
        for which in (0, 1):
            for copy in ring(which, step):
                copy.wait_recv()
            if step < half - 1:
                for copy in ring(which, step + 1):
                    copy.start()

    def hop(d):
        return push(
            q0.at[2, 0],
            q0.at[d, z],
            h_send.at[0, d],
            h_recv.at[0, d],
            {"y": line(sides[d])},
        )

    def q0_straight():
        def go(i, carry):
            for d in range(2):
                push(
                    q0.at[2, 0],
                    q0.at[d, z],
                    q_send.at[0],
                    q_recv.at[0, 0],
                    {"z": plane(far_first(i)), "y": line(sides[d])},
                ).start()
            return carry

        lax.fori_loop(0, nz, go, 0)

    def q0_relay(d):
        def go(i, carry):
            push(
                q0.at[d, z],
                q0.at[d, z],
                q_send.at[0],
                q_recv.at[0, 1],
                {"z": plane(far_first(i))},
            ).start()
            return carry

        lax.fori_loop(0, nz - 1, go, 0)

    def n0_straight():
        def go(i, carry):
            for d in range(2):
                push(
                    nsend0.at[d, i],
                    nrecv0.at[d, z],
                    n0_send,
                    n0_recv,
                    {"z": i, "y": line(-sides[d])},
                ).start()
            return carry

        lax.fori_loop(*groups[0], go, 0)

    def n0_along():
        def go(i, carry):
            @pl.when(i != z)
            def _():
                for d in range(2):
                    push(
                        nsend0.at[d, i], nrecv0.at[d, z], n0_send, n0_recv, {"z": i}
                    ).start()

            return carry

        lax.fori_loop(*groups[1], go, 0)

    def back(d):
        return push(
            back_send.at[d],
            back_recv.at[d],
            b_send.at[d],
            b_recv.at[d],
            {"y": line(-sides[d])},
        )

    early = z < mid

    def wait_group(layer, g, some_of):
        inside = early if g == 0 else jnp.logical_not(early)
        for less, when in ((1, inside), (0, jnp.logical_not(inside))):

            @pl.when(when)
            def _(less=less):
                some = some_of(mid - less)
                push(some, some, q_send.at[layer], q_recv.at[layer, g], {"z": plane(1)}).wait_recv()

    def q1_start():
        def go(i, carry):
            push(
                q1.at[nz],
                q1.at[z],
                q_send.at[1],
                q_recv.at[1, lax.div(z, mid)],
                {"z": plane(far_first(i))},
            ).start()
            return carry

        lax.fori_loop(0, nz - 1, go, 0)

    def n1_start(g):
        def go(i, carry):
            @pl.when(i != z)
            def _():
                push(nsend1.at[i], nrecv1.at[z], n1_send, n1_recv, {"z": i}).start()

            return carry

        lax.fori_loop(*groups[g], go, 0)

    def share_start(layer):
        for k in sorted(range(1, nt), key=lambda k: abs(k - nt // 2)):
            push(
                share.at[layer, lax.rem(t + k, 2)],
                halves.at[layer, nt - k],
                t_send.at[layer],
                t_recv.at[layer],
                {"tp": other(k)},
            ).start()

    waits = []

    def wait_all(ref, send, recv, peer):
        both = push(ref, ref, send, recv, peer)
        both.wait_recv()
        waits.append(both)

    def weigh(layer, queries, keys):
        scores = dot_nt(queries, keys)
        weights = jnp.exp(scl[layer] * (scores * (1.0 / ROOT) - ROOT))
        sums = weights[:, 0:128]
        for c in range(128, weights.shape[1], 128):
            sums = sums + weights[:, c : c + 128]
        return weights.astype(BF16), sums

    def with_denominators(numer, sums):
        count = numer.shape[0]
        denoms = jnp.sum(sums.T, axis=0, keepdims=True)
        upper = denoms.astype(BF16).astype(F32)
        parts = [upper, denoms - upper]
        if count < 128:
            pad = jnp.zeros((1, 128 - count), F32)
            parts = [parts[0], pad, parts[1], pad]
        extra = jnp.concatenate(parts, axis=1).reshape(1, 1, 256)
        shape = (count // PAD, PAD, HEAD_DIM)
        lane = lax.rem(lax.broadcasted_iota(jnp.int32, shape, 2), 128)
        block = lax.broadcasted_iota(jnp.int32, shape, 0)
        row = lax.broadcasted_iota(jnp.int32, shape, 1)
        mine = jnp.where(lane // PAD == block, jnp.broadcast_to(extra, shape), 0.0)
        return jnp.where(row == PAD - 1, mine, numer.reshape(shape)).astype(BF16)

    def share_of(layer, total):
        shape = (PAD, 128)
        lane = lax.broadcasted_iota(jnp.int32, shape, 1)
        row = lax.broadcasted_iota(jnp.int32, shape, 0)
        both = total[PAD - 1 : PAD, 0:128] + total[PAD - 1 : PAD, 128:256]
        denoms = jnp.sum(
            jnp.where(lax.rem(lane, PAD) == row, jnp.broadcast_to(both, shape), 0.0),
            axis=1,
            keepdims=True,
        )
        real = lax.broadcasted_iota(jnp.int32, (PAD, HEAD_DIM), 0) < toks
        attended = jnp.where(real, total / denoms, 0.0).astype(BF16)
        rounded = jnp.dot(attended, wo[layer], preferred_element_type=F32).astype(BF16)
        share[layer, 0] = rounded[:, 0:width]
        share[layer, 1] = rounded[:, width : 2 * width]
        share_start(layer)

    def add_branch(layer):
        wait_all(halves.at[layer, pl.ds(1, nt - 1)], t_send.at[layer], t_recv.at[layer], partner)
        branch = share[layer, core].astype(F32)
        for k in range(1, nt):
            branch = branch + halves[layer, k].astype(F32)
        swap[layer, core] = (hid[core] + branch).astype(BF16)
        both = push(
            swap.at[layer, core], swap.at[layer, core], s_send.at[layer], s_recv.at[layer], partner
        )
        both.start()
        both.wait_recv()
        waits.append(both)

    with scope("queries_0"):
        for i in range(3):
            first[i].wait()
        hid[...] = jnp.zeros_like(hid)
        rows_in = tgt[...].astype(F32)
        hid[0, 0:toks, :] = rows_in[:, 0:width]
        hid[1, 0:toks, :] = rows_in[:, width : 2 * width]
        q0[2, 0] = queries_of(0)
    with scope("norm"):
        first[3].wait()
        first[4].wait()
        lax.fori_loop(0, rows // (2 * step), both_layers, 0)
    with scope("keys_0"):
        first[5].wait()
        kv0[0, 0] = keys_of(0)
    with scope("barrier"):
        pl.semaphore_wait(barrier, greeted)

    @pl.when(early)
    def _():
        q0_straight()

    @pl.when(jnp.logical_not(early))
    def _():
        for d in range(2):
            hop(d).start()

    near(0, 0, 1).start()
    near(0, 0, 3).start()
    with scope("values_0"):
        first[6].wait()
        kv0[1, 0] = values_of(0)
    near(1, 0, 1).start()
    near(1, 0, 3).start()
    with scope("source_1"):
        for i in (0, 1, 2):
            later[i].wait()
        kv1[0, 0] = keys_of(1)
        kv1[1, 0] = values_of(1)
        for i in (3, 4, 5):
            later[i].wait()
    with scope("hop_0"):

        @pl.when(jnp.logical_not(early))
        def _():
            for d in range(2):
                hop(d).wait_recv()
                q0_relay(d)

    for which in (0, 1):
        with scope(f"near_0_{which}"):
            near(which, 0, 1).wait_recv()
            near(which, 1, 2).start()
            near(which, 0, 3).wait_recv()
    for g, (low, high) in enumerate(groups):
        with scope(f"q_wait_0_{g}"):
            some = q0.at[pl.ds(0, 2), pl.ds(low, mid)]
            if g == 0:
                push(some, some, q_send.at[0], q_recv.at[0, 0], {"z": plane(1)}).wait_recv()
            else:
                wait_group(0, g, lambda count, low=low: q0.at[pl.ds(0, 2), pl.ds(low, count)])
        numer = jnp.zeros((2 * tall, HEAD_DIM), F32)
        total = jnp.zeros((2 * tall, 128), F32)
        queries = q0[0:2, low:high].reshape(2 * tall, HEAD_DIM)
        for slot in (0, 1, 3, 2):
            if slot == 2 and g == 0:
                for which in (0, 1):
                    with scope(f"near_1_{which}"):
                        near(which, 1, 2).wait_recv()
                        for copy in ring(which, 0):
                            copy.start()
            with scope(f"attend_0_{g}_{slot}"):
                weights, sums = weigh(0, queries, kv0[0, slot])
                total = total + sums
            numer = numer + jnp.dot(weights, kv0[1, slot], preferred_element_type=F32)
        with scope(f"partials_0_{g}"):
            nsend0[:, low:high] = with_denominators(numer, total).reshape(2, mid, PAD, HEAD_DIM)
            n0_straight() if g == 0 else n0_along()
    with scope("ring_1_0"):
        ring_next(0)
    with scope("ring_late"):

        @pl.when(jnp.logical_not(early))
        def _():
            some = nrecv0.at[pl.ds(0, 2), pl.ds(0, nz - 1)]
            push(some, some, n0_send, n0_recv, {"z": plane(1)}).wait_recv()
            for d in range(2):
                nrecv0[d, z] = nsend0[d, z]
                back_send[d] = jnp.sum(nrecv0[d].astype(F32), axis=0)
                back(d).start()
            ring_next(1)
            for d in range(2):
                back(d).wait_recv()
            gathered[...] = back_recv[0] + back_recv[1]

    with scope("n_wait_0"):

        @pl.when(early)
        def _():
            push(nrecv0, nrecv0, n0_send, n0_recv, {"z": plane(1)}).wait_recv()
            gathered[...] = jnp.sum(
                nrecv0[...].reshape(2 * nz, PAD, HEAD_DIM).astype(F32), axis=0
            )

    with scope("share_0"):
        share_of(0, gathered[...])
    def serve(g):
        low, high = groups[g]
        with scope(f"q_wait_1_{g}"):
            wait_group(1, g, lambda count, low=low: q1.at[pl.ds(low, count)])
        with scope(f"attend_1_{g}"):
            numer = jnp.zeros((tall, HEAD_DIM), F32)
            total = jnp.zeros((tall, 128), F32)
            queries = q1[low:high].reshape(tall, HEAD_DIM)
            for slot in range(0, ny, 2):
                keys = kv1[0, slot : slot + 2].reshape(2 * rows, HEAD_DIM)
                weights, sums = weigh(1, queries, keys)
                total = total + sums
                values = kv1[1, slot : slot + 2].reshape(2 * rows, HEAD_DIM)
                numer = numer + jnp.dot(weights, values, preferred_element_type=F32)
        with scope(f"partials_1_{g}"):
            nsend1[low:high] = with_denominators(numer, total)
            n1_start(g)

    @pl.when(early)
    def _():
        with scope("ring_1_1"):
            ring_next(1)

    @pl.when(jnp.logical_not(early))
    def _():
        with scope("ring_1_2"):
            ring_next(2)

    with scope("t_wait_0"):
        add_branch(0)
    with scope("queries_1"):
        hid[...] = swap[0].astype(F32)
        own = queries_of(1)
        q1[nz] = own
        q1[z] = own
        q1_start()
    @pl.when(early)
    def _():
        ring_next(2)

    with scope("ring_1_3"):
        ring_next(3)
    serve(0)
    serve(1)
    with scope("n_wait_1"):
        nrecv1[z] = nsend1[z]
        some = nrecv1.at[pl.ds(0, nz - 1)]
        wait_all(some, n1_send, n1_recv, {"z": plane(1)})
    with scope("share_1"):
        share_of(1, jnp.sum(nrecv1[...].astype(F32), axis=0))
    with scope("t_wait_1"):
        add_branch(1)
    with scope("drain"):
        out[:, 0:width] = swap[1, 0][0:toks, :]
        out[:, width : 2 * width] = swap[1, 1][0:toks, :]
        for both in waits:
            both.wait_send()

        def sent(layer, some):
            push(
                some, some, q_send.at[layer], q_recv.at[layer, 0], {"z": plane(1)}
            ).wait_send()

        sent(1, q1.at[pl.ds(0, nz - 1)])

        @pl.when(early)
        def _():
            sent(0, q0.at[pl.ds(0, 2)])
            push(nrecv0, nrecv0, n0_send, n0_recv, {"z": plane(1)}).wait_send()

        @pl.when(jnp.logical_not(early))
        def _():
            sent(0, q0.at[pl.ds(0, 2), pl.ds(0, nz - 1)])
            for d in range(2):
                hop(d).wait_send()
                back(d).wait_send()
            some = nsend0.at[pl.ds(0, 2), pl.ds(0, nz - 1)]
            push(some, some, n0_send, n0_recv, {"z": plane(1)}).wait_send()

        for which in (0, 1):
            for held, lands in ((0, 1), (0, 3), (1, 2)):
                near(which, held, lands).wait_send()
            for s in range(half):
                for copy in ring(which, s):
                    copy.wait_send()


def body(sizes, *arrays):
    target, source = arrays[0], arrays[1]
    w_query = arrays[4]
    arrays = (*arrays[:8], arrays[8].reshape(-1))
    nz, ny, nt = sizes
    toks, width = target.shape
    rows = source.shape[0]
    layers = w_query.shape[0]
    half = ny // 2
    hbm = pl.BlockSpec(memory_space=pl.ANY)
    vmem = pltpu.VMEM
    dma = pltpu.SemaphoreType.DMA
    return pl.pallas_call(
        functools.partial(kernel, sizes),
        out_shape=pltpu.VMEM((toks, width), BF16),
        in_specs=[hbm] * 9,
        out_specs=pl.BlockSpec(memory_space=pltpu.VMEM),
        scratch_shapes=[
            vmem((2, PAD, width // 2), F32),
            vmem((rows, width), BF16),
            vmem((rows, 128), F32),
            vmem((toks, width), BF16),
            vmem((layers, width), F32),
            vmem((layers, width), F32),
            vmem((layers, width, HEAD_DIM), BF16),
            vmem((layers, width, HEAD_DIM), BF16),
            vmem((layers, width, HEAD_DIM), BF16),
            vmem((layers, HEAD_DIM, width), BF16),
            pltpu.SMEM((layers,), F32),
            vmem((layers, rows, width), BF16),
            vmem((2, 4, rows, HEAD_DIM), BF16),
            vmem((2, ny, rows, HEAD_DIM), BF16),
            vmem((3, nz, PAD, HEAD_DIM), BF16),
            vmem((nz + 1, PAD, HEAD_DIM), BF16),
            vmem((2, nz, PAD, HEAD_DIM), BF16),
            vmem((2, nz, PAD, HEAD_DIM), BF16),
            vmem((nz, PAD, HEAD_DIM), BF16),
            vmem((nz, PAD, HEAD_DIM), BF16),
            vmem((layers, 2, PAD, width // 2), BF16),
            vmem((2, PAD, HEAD_DIM), F32),
            vmem((2, PAD, HEAD_DIM), F32),
            vmem((PAD, HEAD_DIM), F32),
            vmem((layers, nt, PAD, width // 2), BF16),
            vmem((layers, 2, PAD, width // 2), BF16),
            dma((13,)),
            dma((2, 4)),
            dma((2, 4)),
            dma((2, 2, half)),
            dma((2, ny)),
            dma((layers,)),
            dma((layers, 2)),
            dma((1, 2)),
            dma((1, 2)),
            dma((2,)),
            dma((2,)),
            dma,
            dma,
            dma,
            dma,
            dma((layers,)),
            dma((layers,)),
            dma((layers,)),
            dma((layers,)),
        ],
        compiler_params=pltpu.CompilerParams(collective_id=0, has_side_effects=True),
    )(*arrays)


SP = ("z", "y")


def torus_of(mesh):
    return Mesh(mesh.devices.reshape(16, 8, mesh.shape["tp"]), ("z", "y", "tp"))


def on_torus(torus):
    sizes = tuple(torus.shape[a] for a in ("z", "y", "tp"))
    return jax.shard_map(
        functools.partial(body, sizes),
        mesh=torus,
        in_specs=(
            P(SP, None),
            P(SP, None),
            P(),
            P(),
            P(None, None, "tp"),
            P(None, None, "tp"),
            P(None, None, "tp"),
            P(None, "tp", None),
            P(None, "tp"),
        ),
        out_specs=P(SP, None),
        check_vma=False,
    )


def solution(mesh):
    return on_torus(torus_of(mesh))
```
